256 devices in a mesh: sp: 32 (over z, y), tp: 8 (over x, core).
Axes of the slice: x: 4, y: 4, z: 8, core: 2. Of those that a mesh axis runs over, the one named last changes fastest.
Arguments:
- inputs: bfloat16 [2, 12288, 4096], P(None, 'sp'), may hold values from -8 to 8
- w_key: bfloat16 [4096, 2048], P(None, 'tp'), may hold values from -0.09375 to 0.09375
- w_value: bfloat16 [4096, 2048], P(None, 'tp'), may hold values from -0.09375 to 0.09375
- w_query: bfloat16 [4096, 2048], P(None, 'tp'), may hold values from -0.09375 to 0.09375
- w_igate: bfloat16 [4096, 16], replicated, may hold values from -1 to 1
- w_fgate: bfloat16 [4096, 16], replicated, may hold values from -0.09375 to 0.09375
- forget_bias: float32 [16], replicated, may hold values from 3 to 12
- new_rows: bfloat16 [2, 4096], P(None, 'tp'), may hold values from -6 to 6
Outputs:
- cache_matrix: bfloat16 [2, 16, 128, 128], P(None, 'tp', 'sp')
- cache_normal: float32 [2, 16, 128], P(None, 'tp', 'sp')
- cache_top: float32 [2, 16], P(None, 'tp')
- read: bfloat16 [2, 16, 128], P(None, 'tp', 'sp')
The draws below stay inside these ranges and needn't reach their ends.
All inputs are finite; a program needn't handle non-finite values.
Results may differ from the reference program's by a relative error of at most 0.015.
Values may be sent and summed in bfloat16 or wider, within the bound.
A program may use at most 64 MiB of HBM per device.

```python
import jax
import jax.numpy as jnp
from jax import lax

D = 4096
H = 16
DH = 128
SEQS = 2
LEN = 12288


def draw_inputs(key, part):
    noise_key, shift_key, pick_key, chosen_key = jax.random.split(jax.random.fold_in(key, 3), 4)
    drawn = jax.random.normal(noise_key, (SEQS, LEN, D), jnp.float32)
    shifts = 1.5 * jax.random.normal(shift_key, (SEQS, LEN // 32, 1, D), jnp.float32)
    drawn = drawn + jnp.broadcast_to(shifts, (SEQS, LEN // 32, 32, D)).reshape(SEQS, LEN, D)
    return jnp.clip(drawn, -8.0, 8.0).astype(jnp.bfloat16)


def draw_w_igate(key, part):
    drawn = jax.random.normal(jax.random.fold_in(key, 5), (D, H), jnp.float32) / jnp.sqrt(D * 1.0)
    return jnp.clip(drawn, -1.0, 1.0).astype(jnp.bfloat16)


def draw_forget_bias(key, part):
    pick_key, jitter_key = jax.random.split(jax.random.fold_in(key, 9))
    slow_share = 0.5
    is_slow = jax.random.uniform(pick_key, (H,), jnp.float32) < slow_share
    jitter = jax.random.uniform(jitter_key, (H,), jnp.float32, -0.3, 0.3)
    return jnp.where(is_slow, jnp.log(LEN * 1.0) + 1.0, 3.5) + jitter


def steps_of(rng, dims, cuts, low, top_value):
    level, own = 1.0, jax.random.fold_in(rng, 6)
    for axis_at, blocks in cuts:
        steps = jnp.exp(jax.random.uniform(jax.random.fold_in(own, axis_at), (blocks,), jnp.float32, low / len(cuts), top_value / len(cuts)))
        level = level * jnp.repeat(steps, dims[axis_at] // blocks).reshape([-1 if axis == axis_at else 1 for axis in range(len(dims))])
    return level


def scatter_about(own_key, dims, spread, limit, cuts=(), kind=jnp.bfloat16):
    loudness = steps_of(own_key, dims, cuts, -0.22, 0.18) if cuts else 1.0
    values = jax.random.normal(own_key, dims, jnp.float32) * spread * loudness
    return jnp.minimum(jnp.maximum(values, -limit), limit).astype(kind)


def setup_inputs(seed: int = 0) -> dict:
    seeds = jax.random.split(jax.random.key(seed), 9)
    return {
        "inputs": draw_inputs(jax.random.fold_in(seeds[8], 71), 0),
        "w_key": scatter_about(seeds[1], (D, H * DH), D ** -0.5, 0.09375, ((1, 8),)),
        "w_value": scatter_about(seeds[2], (D, H * DH), D ** -0.5, 0.09375, ((1, 8),)),
        "w_query": scatter_about(seeds[3], (D, H * DH), D ** -0.5, 0.09375, ((1, 8),)),
        "w_igate": draw_w_igate(jax.random.fold_in(seeds[8], 71), 0),
        "w_fgate": scatter_about(seeds[5], (D, H), D ** -0.5, 0.09375),
        "forget_bias": draw_forget_bias(jax.random.fold_in(seeds[8], 71), 0),
        "new_rows": scatter_about(seeds[7], (SEQS, D), 1.0, 6.0, ((1, 8),)),
    }


EPS = 1e-06

def normalize(row_block):
    scaled = row_block.astype(jnp.float32)
    scaled = scaled * lax.rsqrt(lax.optimization_barrier(jnp.mean(scaled * scaled, axis=-1, keepdims=True)) + EPS)
    return scaled.astype(jnp.bfloat16)

def reference(inputs, w_key, w_value, w_query, w_igate, w_fgate, forget_bias, new_rows):

    def per_sequence(row_block):
        normed = normalize(row_block)
        key_heads = jnp.dot(normed, w_key, preferred_element_type=jnp.float32).astype(jnp.bfloat16).reshape(LEN, H, DH)
        value_heads = jnp.dot(normed, w_value, preferred_element_type=jnp.float32).astype(jnp.bfloat16).reshape(LEN, H, DH)
        input_pre = jnp.dot(normed, w_igate, preferred_element_type=jnp.float32)
        log_forget = jax.nn.log_sigmoid(jnp.dot(normed, w_fgate, preferred_element_type=jnp.float32) + forget_bias)
        running = jnp.cumsum(log_forget, axis=0)
        log_weight = running[-1:, :] - running + input_pre
        stabilizer = lax.optimization_barrier(jnp.max(log_weight, axis=0))
        weight = jnp.exp(log_weight - stabilizer[None, :])
        weighted = (weight[:, :, None] * value_heads.astype(jnp.float32)).astype(jnp.bfloat16)
        matrix = jnp.einsum('the,thd->hed', weighted.astype(jnp.float32), key_heads.astype(jnp.float32))
        normal = jnp.einsum('th,thd->hd', weight, key_heads.astype(jnp.float32))
        return (matrix.astype(jnp.bfloat16), normal, stabilizer)
    cache_matrix, cache_normal, cache_top = lax.map(per_sequence, inputs)
    seq_count = new_rows.shape[0]
    new_normed = normalize(new_rows)
    query_new = jnp.dot(new_normed, w_query, preferred_element_type=jnp.float32).astype(jnp.bfloat16)
    key_new = jnp.dot(new_normed, w_key, preferred_element_type=jnp.float32).astype(jnp.bfloat16)
    value_new = jnp.dot(new_normed, w_value, preferred_element_type=jnp.float32).astype(jnp.bfloat16)
    query_new = query_new.astype(jnp.float32).reshape(seq_count, H, DH)
    key_new = key_new.astype(jnp.float32).reshape(seq_count, H, DH)
    value_new = value_new.astype(jnp.float32).reshape(seq_count, H, DH)
    input_new = jnp.dot(new_normed, w_igate, preferred_element_type=jnp.float32)
    forget_new = jax.nn.log_sigmoid(jnp.dot(new_normed, w_fgate, preferred_element_type=jnp.float32) + forget_bias)
    top_next = jnp.maximum(forget_new + cache_top, input_new)
    old_share = jnp.exp(forget_new + cache_top - top_next)
    new_share = jnp.exp(input_new - top_next)
    agreement = lax.optimization_barrier(jnp.sum(key_new * query_new, axis=-1))
    factor = DH ** (-0.5)
    numerator = old_share[..., None] * jnp.einsum('shed,shd->she', cache_matrix.astype(jnp.float32), query_new)
    numerator = (numerator + (new_share * agreement)[..., None] * value_new) * factor
    denominator = (old_share * lax.optimization_barrier(jnp.sum(cache_normal * query_new, axis=-1)) + new_share * agreement) * factor
    read = numerator / jnp.maximum(jnp.abs(denominator), 1.0)[..., None]
    return (cache_matrix, cache_normal, cache_top, read.astype(jnp.bfloat16))
```

```python
import functools

import jax
import jax.numpy as jnp
from jax import lax
from jax.experimental import pallas as pl
from jax.experimental.pallas import tpu as pltpu
from jax.sharding import PartitionSpec as P

DH = 128
EPS = 1e-06
MESH = pl.DeviceIdType.MESH
F32 = jnp.float32
BF16 = jnp.bfloat16
NZ, NY = 8, 4
SP, TP = NZ * NY, 8
CHUNKS = 2
BLOCKS = ((0, 128), (128, 256), (384, 384))
MSG = 24


def peer_offsets():
    offsets = [(dz, dy) for dz in range(NZ) for dy in range(NY) if dz or dy]
    return sorted(offsets, key=lambda o: -(min(o[0], NZ - o[0]) + min(o[1], NY - o[1])))


def iota(shape, dim):
    return lax.broadcasted_iota(jnp.int32, shape, dim)


def log_sigmoid(v):
    u = jnp.exp(-jnp.abs(v))
    series = u * (1.0 - u * (0.5 - u * (1.0 / 3.0 - u * (0.25 - u * (0.2 - u * (1.0 / 6.0))))))
    return jnp.minimum(v, 0.0) - jnp.where(u < 0.03, series, jnp.log(1.0 + u))


def split3(v):
    hi = v.astype(BF16).astype(F32)
    rest = v - hi
    mid = rest.astype(BF16).astype(F32)
    return hi, mid, rest - mid


def kernel(
    x_hbm, wk_hbm, wv_hbm, wq_hbm, wi_hbm, wf_hbm, bias_hbm, new_hbm,
    mat_out, nrm_out, top_out, read_out,
    x, xn, wk, wv, wq, wg, bias, fresh, keys, values, acc_g, tri, wrow, stat,
    send_m, recv_m, send_s, recv_s,
    load_sem, x_sem, w_sem, new_sem, msem, ssem,
):
    sp, tp = lax.axis_index("sp"), lax.axis_index("tp")
    z, y = sp // NY, lax.rem(sp, NY)
    rows, width = x.shape
    span = rows // 2
    step = width // CHUNKS
    peers = []
    for dz, dy in peer_offsets():
        peers.append(lax.rem(z + dz, NZ) * NY + lax.rem(y + dy, NY))
    tp_peers = [lax.rem(tp + k, TP) for k in range(1, TP)]

    small = [
        pltpu.make_async_copy(wi_hbm, wg.at[pl.ds(0, 16)], load_sem.at[0]),
        pltpu.make_async_copy(wf_hbm, wg.at[pl.ds(16, 16)], load_sem.at[1]),
        pltpu.make_async_copy(bias_hbm, bias, load_sem.at[2]),
        pltpu.make_async_copy(new_hbm, fresh.at[tp], load_sem.at[3]),
    ]
    x_loads = []
    for i, (at, count) in enumerate(BLOCKS):
        part = pl.ds(at, count)
        x_loads.append(pltpu.make_async_copy(x_hbm.at[part], x.at[part], x_sem.at[i]))
    w_loads = []
    for c in range(CHUNKS):
        part = pl.ds(c * step, step)
        w_loads.append(pltpu.make_async_copy(wv_hbm.at[part], wv.at[part], w_sem.at[c, 0]))
        w_loads.append(pltpu.make_async_copy(wk_hbm.at[part], wk.at[part], w_sem.at[c, 1]))
    load_q = pltpu.make_async_copy(wq_hbm, wq, load_sem.at[4])
    for copy in (x_loads[0], *small, *w_loads, *x_loads[1:], load_q):
        copy.start()

    barrier = pltpu.get_barrier_semaphore()
    for p in peers:
        pl.semaphore_signal(barrier, inc=1, device_id=(p, tp), device_id_type=MESH)
    for p in tp_peers:
        pl.semaphore_signal(barrier, inc=1, device_id=(sp, p), device_id_type=MESH)

    tri[...] = (iota((span, span), 0) > iota((span, span), 1)).astype(F32).astype(BF16)
    for copy in small:
        copy.wait()
    eye = iota((16, 128), 0) == iota((16, 128), 1)
    bias_row = jnp.concatenate([bias[...], jnp.zeros((1, 112), F32)], axis=1)
    bias_col = jnp.sum(jnp.where(eye, bias_row, 0.0), axis=1, keepdims=True)

    def normalise(i):
        at, count = BLOCKS[i]
        total = None
        for c in range(0, width, 128):
            piece = x[at:at + count, c:c + 128].astype(F32)
            total = piece * piece if total is None else total + piece * piece
        r = lax.rsqrt(jnp.sum(total, axis=1, keepdims=True) * (1.0 / width) + EPS)
        for c in range(0, width, 128):
            xn[at:at + count, c:c + 128] = (x[at:at + count, c:c + 128].astype(F32) * r).astype(BF16)

    def project(i):
        at, count = BLOCKS[i]
        rows_n = xn[at:at + count, :]
        acc_g[at:at + count, 0:32] = lax.dot_general(
            rows_n, wg[...], (((1,), (1,)), ((), ())), preferred_element_type=F32
        )
        values[at:at + count, :] = jnp.dot(rows_n, wv[...], preferred_element_type=F32).astype(BF16)
        keys[at:at + count, :] = jnp.dot(rows_n, wk[...], preferred_element_type=F32).astype(BF16)

    x_loads[0].wait()
    normalise(0)
    for copy in w_loads:
        copy.wait()
    for i in range(1, len(BLOCKS)):
        x_loads[i].wait()
        normalise(i)
        project(i - 1)
    project(len(BLOCKS) - 1)

    gates = []
    for s in range(2):
        turned = acc_g[pl.ds(s * span, span), :].T
        gates.append((turned[0:16], log_sigmoid(turned[16:32] + bias_col)))
    parts = [split3(g[1]) for g in gates]
    lhs = jnp.concatenate([p[i] for p in parts for i in range(3)], axis=0).astype(BF16)
    after = jnp.dot(lhs, tri[...], preferred_element_type=F32)
    for s in range(2):
        igate, logf = gates[s]
        rest = after[48 * s:48 * s + 16] + after[48 * s + 16:48 * s + 32] + after[48 * s + 32:48 * s + 48]
        logw = rest + igate
        top = jnp.max(logw, axis=1, keepdims=True)
        wrow[pl.ds(16 * s, 16), :] = jnp.exp(logw - top)
        stat[0, pl.ds(16 * s, 16), :] = jnp.broadcast_to(rest[:, 0:1] + logf[:, 0:1], (16, 128))
        stat[1, pl.ds(16 * s, 16), :] = jnp.broadcast_to(top, (16, 128))

    lane = iota((1, 128), 1)
    lane_q = jnp.where(lane < 16, lane // 4, jnp.where(lane < MSG, lax.rem(lane, 4), -1))
    for i in range(2):
        line = jnp.zeros((1, 128), F32)
        for q in range(4):
            own = stat[i, pl.ds(16 * (q // 2) + 2 * tp + q % 2, 1), :]
            line = jnp.where(lane_q == q, own, line)
        send_s[pl.ds(i, 1), :] = line
    recv_s[sp] = send_s[...]

    pl.semaphore_wait(barrier, SP - 1 + TP - 1)
    s_copies, m_copies, n_copies = [], [], []
    for p in peers:
        copy = pltpu.make_async_remote_copy(
            src_ref=send_s, dst_ref=recv_s.at[sp], send_sem=ssem.at[0], recv_sem=ssem.at[1],
            device_id=(p, tp), device_id_type=MESH,
        )
        copy.start()
    for p in tp_peers:
        copy = pltpu.make_async_remote_copy(
            src_ref=fresh.at[tp], dst_ref=fresh.at[tp], send_sem=new_sem.at[0], recv_sem=new_sem.at[1],
            device_id=(sp, p), device_id_type=MESH,
        )
        copy.start()

    mats, nrms = [], []
    for q in range(4):
        s, h = q // 2, q % 2
        w = wrow[pl.ds(16 * s + 2 * tp + h, 1), :]
        block, cols = pl.ds(s * span, span), slice(h * DH, (h + 1) * DH)
        turned = (values[block, cols].T.astype(F32) * w).astype(BF16)
        hi, mid, low = split3(w)
        row = iota((16, span), 0)
        extra = jnp.where(row == 0, hi, jnp.where(row == 1, mid, jnp.where(row == 2, low, 0.0)))
        out = jnp.dot(
            jnp.concatenate([turned, extra.astype(BF16)], axis=0),
            keys[block, cols],
            preferred_element_type=F32,
        )
        mats.append(out[0:128].reshape(16, 8, 128))
        nrms.append(out[128:129] + out[129:130] + out[130:131])

    low_half = iota((16, 8, 128), 1) < 4
    evens, odds = [], []
    for a, b in ((mats[0], mats[1]), (mats[2], mats[3])):
        evens.append(jnp.where(low_half, a, pltpu.roll(b, 4, 1)))
        odds.append(jnp.where(low_half, pltpu.roll(a, 4, 1), b))
    row8 = iota((8, 128), 0)
    tail = jnp.zeros((8, 128), F32)
    for q in range(4):
        hi = nrms[q].astype(BF16).astype(F32)
        tail = jnp.where(row8 == q, hi, jnp.where(row8 == 4 + q, nrms[q] - hi, tail))
    tail = jnp.broadcast_to(tail[None], (16, 8, 128))
    send_m[:, 0] = jnp.concatenate([evens[0], evens[1], tail], axis=1).astype(BF16)
    send_m[:, 1] = jnp.concatenate([odds[0], odds[1], tail], axis=1).astype(BF16)
    for p in peers:
        copy = pltpu.make_async_remote_copy(
            src_ref=send_m.at[p // 2, lax.rem(p, 2)], dst_ref=recv_m.at[sp],
            send_sem=msem.at[0], recv_sem=msem.at[1], device_id=(p, tp), device_id_type=MESH,
        )
        copy.start()
    recv_m[sp] = send_m[sp // 2, lax.rem(sp, 2)]

    got = fresh.at[pl.ds(0, TP - 1)]
    pltpu.make_async_copy(got, got, new_sem.at[1]).wait()
    pieces = [fresh[k].astype(F32) for k in range(TP)]
    fresh_row = jnp.concatenate(pieces, axis=1)
    mean = jnp.sum(fresh_row * fresh_row, axis=1, keepdims=True) * (1.0 / width)
    token = (fresh_row * lax.rsqrt(mean + EPS)).astype(BF16)
    load_q.wait()
    key = jnp.dot(token, wk[...], preferred_element_type=F32).astype(BF16).astype(F32)
    value = jnp.dot(token, wv[...], preferred_element_type=F32).astype(BF16).astype(F32)
    query = jnp.dot(token, wq[...], preferred_element_type=F32).astype(BF16).astype(F32)
    gate = lax.dot_general(token, wg[...], (((1,), (1,)), ((), ())), preferred_element_type=F32)

    def per_row(v):
        return jnp.concatenate(
            [
                jnp.broadcast_to(v[q // 2:q // 2 + 1, (q % 2) * DH:(q % 2 + 1) * DH], (4, DH))
                for q in range(4)
            ],
            axis=0,
        )

    def picked(v, at):
        return jnp.sum(jnp.where(iota((16, v.shape[1]), 1) == at, v, 0.0), axis=1, keepdims=True)

    row16 = iota((16, 1), 0)
    own_row = 4 * sp + lax.rem(row16, 4)
    head = 2 * tp + lax.rem(row16 // 4, 2)
    q_rows, k_rows, v_rows = per_row(query), per_row(key), per_row(value)
    agreement = jnp.sum(q_rows * k_rows, axis=1, keepdims=True)
    value_own = picked(v_rows, own_row)
    gate_rows = jnp.concatenate([jnp.broadcast_to(gate[s:s + 1], (8, 32)) for s in range(2)], axis=0)
    input_new = picked(gate_rows, head)
    bias_own = picked(jnp.broadcast_to(bias_row, (16, 128)), head)
    forget_new = log_sigmoid(picked(gate_rows, 16 + head) + bias_own)

    got = recv_s.at[pl.ds(0, SP - 1)]
    pltpu.make_async_copy(got, got, ssem.at[1]).wait()
    totals, tops = recv_s[:, 0, :], recv_s[:, 1, :]
    later = (iota((SP, SP), 1) > iota((SP, SP), 0)).astype(F32).astype(BF16)
    sums = jnp.dot(later, jnp.concatenate(split3(totals), axis=1).astype(BF16), preferred_element_type=F32)
    lw = sums[:, 0:128] + sums[:, 128:256] + sums[:, 256:384] + tops
    top = jnp.max(lw, axis=0, keepdims=True)
    scale = jnp.exp(lw - top)
    stacked = jnp.concatenate([scale, jnp.broadcast_to(top, (8, 128)), jnp.zeros((88, 128), F32)], axis=0)
    turned = stacked.T
    top_col = turned[0:16, SP:SP + 1]
    share = turned[0:MSG, 0:SP]
    top_next = jnp.maximum(forget_new + top_col, input_new)
    old_share = jnp.exp(forget_new + top_col - top_next)
    new_share = jnp.exp(input_new - top_next)

    got = recv_m.at[pl.ds(0, SP - 1)]
    pltpu.make_async_copy(got, got, msem.at[1]).wait()
    merged = jnp.zeros((MSG, 128), F32)
    for d in range(SP):
        merged = merged + share[:, d:d + 1] * recv_m[d].astype(F32)
    matrix = merged[0:16].astype(BF16)
    normal = merged[16:24] + pltpu.roll(merged[16:24], 4, 0)
    n_rows = jnp.concatenate([jnp.broadcast_to(normal[q:q + 1], (4, 128)) for q in range(4)], axis=0)

    factor = DH ** (-0.5)
    numer = jnp.sum(matrix.astype(F32) * q_rows, axis=1, keepdims=True)
    numer = (old_share * numer + new_share * agreement * value_own) * factor
    denom = jnp.sum(n_rows * q_rows, axis=1, keepdims=True)
    denom = (old_share * denom + new_share * agreement) * factor
    read = numer / jnp.maximum(jnp.abs(denom), 1.0)
    own_normal = picked(n_rows, own_row)

    lane16 = iota((16, 128), 1)
    table = jnp.where(lane16 == 0, own_normal, jnp.where(lane16 == 1, top_col, read))
    table = jnp.concatenate([table, jnp.zeros((112, 128), F32)], axis=0).T
    for q in range(4):
        s, h = q // 2, q % 2
        mat_out[s, h] = matrix[4 * q:4 * q + 4]
        nrm_out[s, h:h + 1, :] = table[0:1, 4 * q:4 * q + 4]
        top_out[s:s + 1, h:h + 1] = table[1:2, 4 * q:4 * q + 1]
        read_out[s, h:h + 1, :] = table[2:3, 4 * q:4 * q + 4].astype(BF16)

    sent = recv_s.at[pl.ds(0, SP - 1)]
    pltpu.make_async_copy(sent, sent, ssem.at[0]).wait()
    sent = recv_m.at[pl.ds(0, SP - 1)]
    pltpu.make_async_copy(sent, sent, msem.at[0]).wait()
    sent = fresh.at[pl.ds(0, TP - 1)]
    pltpu.make_async_copy(sent, sent, new_sem.at[0]).wait()


def shards(inputs, w_key, w_value, w_query, w_igate, w_fgate, forget_bias, new_rows):
    seqs, span, width = inputs.shape
    rows = seqs * span
    heads = w_key.shape[1] // DH
    out_shape = (
        jax.ShapeDtypeStruct((seqs, heads, DH // SP, DH), BF16),
        jax.ShapeDtypeStruct((seqs, heads, DH // SP), F32),
        jax.ShapeDtypeStruct((seqs, heads), F32),
        jax.ShapeDtypeStruct((seqs, heads, DH // SP), BF16),
    )
    hbm = pl.BlockSpec(memory_space=pl.ANY)
    vmem = pl.BlockSpec(memory_space=pltpu.VMEM)
    dma = pltpu.SemaphoreType.DMA
    return pl.pallas_call(
        kernel,
        out_shape=out_shape,
        in_specs=[hbm] * 8,
        out_specs=[vmem] * 4,
        scratch_shapes=[
            pltpu.VMEM((rows, width), BF16),
            pltpu.VMEM((rows, width), BF16),
            pltpu.VMEM((width, heads * DH), BF16),
            pltpu.VMEM((width, heads * DH), BF16),
            pltpu.VMEM((width, heads * DH), BF16),
            pltpu.VMEM((32, width), BF16),
            pltpu.VMEM((1, 16), F32),
            pltpu.VMEM((TP, seqs, width // TP), BF16),
            pltpu.VMEM((rows, heads * DH), BF16),
            pltpu.VMEM((rows, heads * DH), BF16),
            pltpu.VMEM((rows, 128), F32),
            pltpu.VMEM((span, span), BF16),
            pltpu.VMEM((2 * 16, span), F32),
            pltpu.VMEM((2, 2 * 16, 128), F32),
            pltpu.VMEM((SP // 2, 2, MSG, 128), BF16),
            pltpu.VMEM((SP, MSG, 128), BF16),
            pltpu.VMEM((2, 128), F32),
            pltpu.VMEM((SP, 2, 128), F32),
            dma((5,)),
            dma((len(BLOCKS),)),
            dma((CHUNKS, 2)),
            dma((2,)),
            dma((2,)),
            dma((2,)),
        ],
        compiler_params=pltpu.CompilerParams(
            collective_id=0, has_side_effects=True, vmem_limit_bytes=60 * 1024 * 1024
        ),
    )(
        inputs.reshape(rows, width), w_key, w_value, w_query,
        w_igate.T, w_fgate.T, forget_bias.reshape(1, -1), new_rows,
    )


def solution(mesh):
    in_specs = (
        P(None, "sp", None),
        P(None, "tp"),
        P(None, "tp"),
        P(None, "tp"),
        P(),
        P(),
        P(),
        P(None, "tp"),
    )
    out_specs = (P(None, "tp", "sp", None), P(None, "tp", "sp"), P(None, "tp"), P(None, "tp", "sp"))
    return jax.shard_map(shards, mesh=mesh, in_specs=in_specs, out_specs=out_specs, check_vma=False)
```

```python
import functools

import jax
import jax.numpy as jnp
from jax import lax
from jax.experimental import pallas as pl
from jax.experimental.pallas import tpu as pltpu
from jax.sharding import PartitionSpec as P

DH = 128
EPS = 1e-06
MESH = pl.DeviceIdType.MESH
F32 = jnp.float32
BF16 = jnp.bfloat16
NZ, NY = 8, 4
SP, TP = NZ * NY, 8
CHUNKS = 2
BLOCKS = ((0, 128), (128, 256), (384, 384))
MSG = 24


def peer_offsets():
    offsets = [(dz, dy) for dz in range(NZ) for dy in range(NY) if dz or dy]
    return sorted(offsets, key=lambda o: -(min(o[0], NZ - o[0]) + min(o[1], NY - o[1])))


def iota(shape, dim):
    return lax.broadcasted_iota(jnp.int32, shape, dim)


def log_sigmoid(v):
    u = jnp.exp(-jnp.abs(v))
    series = u * (1.0 - u * (0.5 - u * (1.0 / 3.0 - u * (0.25 - u * (0.2 - u * (1.0 / 6.0))))))
    return jnp.minimum(v, 0.0) - jnp.where(u < 0.03, series, jnp.log(1.0 + u))


def split3(v):
    hi = v.astype(BF16).astype(F32)
    rest = v - hi
    mid = rest.astype(BF16).astype(F32)
    return hi, mid, rest - mid


def kernel(
    x_hbm, wk_hbm, wv_hbm, wq_hbm, wi_hbm, wf_hbm, bias_hbm, new_hbm,
    packed_out,
    x, xn, wk, wv, wq, wg, bias, fresh, keys, values, acc_g, tri, wrow, stat,
    send_m, recv_m, send_s, recv_s,
    load_sem, x_sem, w_sem, new_sem, msem, ssem,
):
    sp, tp = lax.axis_index("sp"), lax.axis_index("tp")
    z, y = sp // NY, lax.rem(sp, NY)
    rows, width = x.shape
    span = rows // 2
    step = width // CHUNKS
    peers = []
    for dz, dy in peer_offsets():
        peers.append(lax.rem(z + dz, NZ) * NY + lax.rem(y + dy, NY))
    tp_peers = [lax.rem(tp + k, TP) for k in range(1, TP)]

    small = [
        pltpu.make_async_copy(wi_hbm, wg.at[pl.ds(0, 16)], load_sem.at[0]),
        pltpu.make_async_copy(wf_hbm, wg.at[pl.ds(16, 16)], load_sem.at[1]),
        pltpu.make_async_copy(bias_hbm, bias, load_sem.at[2]),
        pltpu.make_async_copy(new_hbm, fresh.at[tp], load_sem.at[3]),
    ]
    x_loads = []
    for i, (at, count) in enumerate(BLOCKS):
        part = pl.ds(at, count)
        x_loads.append(pltpu.make_async_copy(x_hbm.at[part], x.at[part], x_sem.at[i]))
    w_loads = []
    for c in range(CHUNKS):
        part = pl.ds(c * step, step)
        w_loads.append(pltpu.make_async_copy(wv_hbm.at[part], wv.at[part], w_sem.at[c, 0]))
        w_loads.append(pltpu.make_async_copy(wk_hbm.at[part], wk.at[part], w_sem.at[c, 1]))
    load_q = pltpu.make_async_copy(wq_hbm, wq, load_sem.at[4])
    for copy in (x_loads[0], *small, *w_loads, *x_loads[1:], load_q):
        copy.start()

    barrier = pltpu.get_barrier_semaphore()
    for p in peers:
        pl.semaphore_signal(barrier, inc=1, device_id=(p, tp), device_id_type=MESH)
    for p in tp_peers:
        pl.semaphore_signal(barrier, inc=1, device_id=(sp, p), device_id_type=MESH)

    tri[...] = (iota((span, span), 0) > iota((span, span), 1)).astype(F32).astype(BF16)
    for copy in small:
        copy.wait()
    eye = iota((16, 128), 0) == iota((16, 128), 1)
    bias_row = jnp.concatenate([bias[...], jnp.zeros((1, 112), F32)], axis=1)
    bias_col = jnp.sum(jnp.where(eye, bias_row, 0.0), axis=1, keepdims=True)

    def normalise(i):
        at, count = BLOCKS[i]
        total = None
        for c in range(0, width, 128):
            piece = x[at:at + count, c:c + 128].astype(F32)
            total = piece * piece if total is None else total + piece * piece
        r = lax.rsqrt(jnp.sum(total, axis=1, keepdims=True) * (1.0 / width) + EPS)
        for c in range(0, width, 128):
            xn[at:at + count, c:c + 128] = (x[at:at + count, c:c + 128].astype(F32) * r).astype(BF16)

    def project(i):
        at, count = BLOCKS[i]
        rows_n = xn[at:at + count, :]
        acc_g[at:at + count, 0:32] = lax.dot_general(
            rows_n, wg[...], (((1,), (1,)), ((), ())), preferred_element_type=F32
        )
        values[at:at + count, :] = jnp.dot(rows_n, wv[...], preferred_element_type=F32).astype(BF16)
        keys[at:at + count, :] = jnp.dot(rows_n, wk[...], preferred_element_type=F32).astype(BF16)

    x_loads[0].wait()
    normalise(0)
    for copy in w_loads:
        copy.wait()
    for i in range(1, len(BLOCKS)):
        x_loads[i].wait()
        normalise(i)
        project(i - 1)
    project(len(BLOCKS) - 1)

    gates = []
    for s in range(2):
        turned = acc_g[pl.ds(s * span, span), :].T
        gates.append((turned[0:16], log_sigmoid(turned[16:32] + bias_col)))
    parts = [split3(g[1]) for g in gates]
    lhs = jnp.concatenate([p[i] for p in parts for i in range(3)], axis=0).astype(BF16)
    after = jnp.dot(lhs, tri[...], preferred_element_type=F32)
    for s in range(2):
        igate, logf = gates[s]
        rest = after[48 * s:48 * s + 16] + after[48 * s + 16:48 * s + 32] + after[48 * s + 32:48 * s + 48]
        logw = rest + igate
        top = jnp.max(logw, axis=1, keepdims=True)
        wrow[pl.ds(16 * s, 16), :] = jnp.exp(logw - top)
        stat[0, pl.ds(16 * s, 16), :] = jnp.broadcast_to(rest[:, 0:1] + logf[:, 0:1], (16, 128))
        stat[1, pl.ds(16 * s, 16), :] = jnp.broadcast_to(top, (16, 128))

    lane = iota((1, 128), 1)
    lane_q = jnp.where(lane < 16, lane // 4, jnp.where(lane < MSG, lax.rem(lane, 4), -1))
    for i in range(2):
        line = jnp.zeros((1, 128), F32)
        for q in range(4):
            own = stat[i, pl.ds(16 * (q // 2) + 2 * tp + q % 2, 1), :]
            line = jnp.where(lane_q == q, own, line)
        send_s[pl.ds(i, 1), :] = line
    recv_s[sp] = send_s[...]

    pl.semaphore_wait(barrier, SP - 1 + TP - 1)
    s_copies, m_copies, n_copies = [], [], []
    for p in peers:
        copy = pltpu.make_async_remote_copy(
            src_ref=send_s, dst_ref=recv_s.at[sp], send_sem=ssem.at[0], recv_sem=ssem.at[1],
            device_id=(p, tp), device_id_type=MESH,
        )
        copy.start()
    for p in tp_peers:
        copy = pltpu.make_async_remote_copy(
            src_ref=fresh.at[tp], dst_ref=fresh.at[tp], send_sem=new_sem.at[0], recv_sem=new_sem.at[1],
            device_id=(sp, p), device_id_type=MESH,
        )
        copy.start()

    mats, nrms = [], []
    for q in range(4):
        s, h = q // 2, q % 2
        w = wrow[pl.ds(16 * s + 2 * tp + h, 1), :]
        block, cols = pl.ds(s * span, span), slice(h * DH, (h + 1) * DH)
        turned = (values[block, cols].T.astype(F32) * w).astype(BF16)
        hi, mid, low = split3(w)
        row = iota((16, span), 0)
        extra = jnp.where(row == 0, hi, jnp.where(row == 1, mid, jnp.where(row == 2, low, 0.0)))
        out = jnp.dot(
            jnp.concatenate([turned, extra.astype(BF16)], axis=0),
            keys[block, cols],
            preferred_element_type=F32,
        )
        mats.append(out[0:128].reshape(16, 8, 128))
        nrms.append(out[128:129] + out[129:130] + out[130:131])

    low_half = iota((16, 8, 128), 1) < 4
    evens, odds = [], []
    for a, b in ((mats[0], mats[1]), (mats[2], mats[3])):
        evens.append(jnp.where(low_half, a, pltpu.roll(b, 4, 1)))
        odds.append(jnp.where(low_half, pltpu.roll(a, 4, 1), b))
    row8 = iota((8, 128), 0)
    tail = jnp.zeros((8, 128), F32)
    for q in range(4):
        hi = nrms[q].astype(BF16).astype(F32)
        tail = jnp.where(row8 == q, hi, jnp.where(row8 == 4 + q, nrms[q] - hi, tail))
    tail = jnp.broadcast_to(tail[None], (16, 8, 128))
    send_m[:, 0] = jnp.concatenate([evens[0], evens[1], tail], axis=1).astype(BF16)
    send_m[:, 1] = jnp.concatenate([odds[0], odds[1], tail], axis=1).astype(BF16)
    for p in peers:
        copy = pltpu.make_async_remote_copy(
            src_ref=send_m.at[p // 2, lax.rem(p, 2)], dst_ref=recv_m.at[sp],
            send_sem=msem.at[0], recv_sem=msem.at[1], device_id=(p, tp), device_id_type=MESH,
        )
        copy.start()
    recv_m[sp] = send_m[sp // 2, lax.rem(sp, 2)]

    got = fresh.at[pl.ds(0, TP - 1)]
    pltpu.make_async_copy(got, got, new_sem.at[1]).wait()
    pieces = [fresh[k].astype(F32) for k in range(TP)]
    fresh_row = jnp.concatenate(pieces, axis=1)
    mean = jnp.sum(fresh_row * fresh_row, axis=1, keepdims=True) * (1.0 / width)
    token = (fresh_row * lax.rsqrt(mean + EPS)).astype(BF16)
    load_q.wait()
    key = jnp.dot(token, wk[...], preferred_element_type=F32).astype(BF16).astype(F32)
    value = jnp.dot(token, wv[...], preferred_element_type=F32).astype(BF16).astype(F32)
    query = jnp.dot(token, wq[...], preferred_element_type=F32).astype(BF16).astype(F32)
    gate = lax.dot_general(token, wg[...], (((1,), (1,)), ((), ())), preferred_element_type=F32)

    def per_row(v):
        return jnp.concatenate(
            [
                jnp.broadcast_to(v[q // 2:q // 2 + 1, (q % 2) * DH:(q % 2 + 1) * DH], (4, DH))
                for q in range(4)
            ],
            axis=0,
        )

    def picked(v, at):
        return jnp.sum(jnp.where(iota((16, v.shape[1]), 1) == at, v, 0.0), axis=1, keepdims=True)

    row16 = iota((16, 1), 0)
    own_row = 4 * sp + lax.rem(row16, 4)
    head = 2 * tp + lax.rem(row16 // 4, 2)
    q_rows, k_rows, v_rows = per_row(query), per_row(key), per_row(value)
    agreement = jnp.sum(q_rows * k_rows, axis=1, keepdims=True)
    value_own = picked(v_rows, own_row)
    gate_rows = jnp.concatenate([jnp.broadcast_to(gate[s:s + 1], (8, 32)) for s in range(2)], axis=0)
    input_new = picked(gate_rows, head)
    bias_own = picked(jnp.broadcast_to(bias_row, (16, 128)), head)
    forget_new = log_sigmoid(picked(gate_rows, 16 + head) + bias_own)

    got = recv_s.at[pl.ds(0, SP - 1)]
    pltpu.make_async_copy(got, got, ssem.at[1]).wait()
    totals, tops = recv_s[:, 0, :], recv_s[:, 1, :]
    later = (iota((SP, SP), 1) > iota((SP, SP), 0)).astype(F32).astype(BF16)
    sums = jnp.dot(later, jnp.concatenate(split3(totals), axis=1).astype(BF16), preferred_element_type=F32)
    lw = sums[:, 0:128] + sums[:, 128:256] + sums[:, 256:384] + tops
    top = jnp.max(lw, axis=0, keepdims=True)
    scale = jnp.exp(lw - top)
    stacked = jnp.concatenate([scale, jnp.broadcast_to(top, (8, 128)), jnp.zeros((88, 128), F32)], axis=0)
    turned = stacked.T
    top_col = turned[0:16, SP:SP + 1]
    share = turned[0:MSG, 0:SP]
    top_next = jnp.maximum(forget_new + top_col, input_new)
    old_share = jnp.exp(forget_new + top_col - top_next)
    new_share = jnp.exp(input_new - top_next)

    got = recv_m.at[pl.ds(0, SP - 1)]
    pltpu.make_async_copy(got, got, msem.at[1]).wait()
    merged = jnp.zeros((MSG, 128), F32)
    for d in range(SP):
        merged = merged + share[:, d:d + 1] * recv_m[d].astype(F32)
    matrix = merged[0:16].astype(BF16)
    normal = merged[16:24] + pltpu.roll(merged[16:24], 4, 0)
    n_rows = jnp.concatenate([jnp.broadcast_to(normal[q:q + 1], (4, 128)) for q in range(4)], axis=0)

    factor = DH ** (-0.5)
    numer = jnp.sum(matrix.astype(F32) * q_rows, axis=1, keepdims=True)
    numer = (old_share * numer + new_share * agreement * value_own) * factor
    denom = jnp.sum(n_rows * q_rows, axis=1, keepdims=True)
    denom = (old_share * denom + new_share * agreement) * factor
    read = numer / jnp.maximum(jnp.abs(denom), 1.0)
    own_normal = picked(n_rows, own_row)

    lane16 = iota((16, 128), 1)
    table = jnp.where(lane16 == 0, own_normal, jnp.where(lane16 == 1, top_col, read))
    table = jnp.concatenate([table, jnp.zeros((112, 128), F32)], axis=0).T
    packed_out[0:16] = merged[0:16]
    packed_out[16:24] = table[0:8]

    sent = recv_s.at[pl.ds(0, SP - 1)]
    pltpu.make_async_copy(sent, sent, ssem.at[0]).wait()
    sent = recv_m.at[pl.ds(0, SP - 1)]
    pltpu.make_async_copy(sent, sent, msem.at[0]).wait()
    sent = fresh.at[pl.ds(0, TP - 1)]
    pltpu.make_async_copy(sent, sent, new_sem.at[0]).wait()


def unpack(packed, mat_out, nrm_out, top_out, read_out):
    for q in range(4):
        s, h = q // 2, q % 2
        lanes = slice(4 * q, 4 * q + 4)
        mat_out[s, h] = packed[lanes].astype(BF16)
        nrm_out[s, h:h + 1, :] = packed[16:17, lanes]
        top_out[s:s + 1, h:h + 1] = packed[17:18, 4 * q:4 * q + 1]
        read_out[s, h:h + 1, :] = packed[18:19, lanes].astype(BF16)


def shards(inputs, w_key, w_value, w_query, w_igate, w_fgate, forget_bias, new_rows):
    seqs, span, width = inputs.shape
    rows = seqs * span
    heads = w_key.shape[1] // DH
    out_shape = (
        jax.ShapeDtypeStruct((seqs, heads, DH // SP, DH), BF16),
        jax.ShapeDtypeStruct((seqs, heads, DH // SP), F32),
        jax.ShapeDtypeStruct((seqs, heads), F32),
        jax.ShapeDtypeStruct((seqs, heads, DH // SP), BF16),
    )
    hbm = pl.BlockSpec(memory_space=pl.ANY)
    vmem = pl.BlockSpec(memory_space=pltpu.VMEM)
    dma = pltpu.SemaphoreType.DMA
    packed = pl.pallas_call(
        kernel,
        out_shape=pltpu.VMEM((MSG, 128), F32),
        in_specs=[hbm] * 8,
        out_specs=vmem,
        scratch_shapes=[
            pltpu.VMEM((rows, width), BF16),
            pltpu.VMEM((rows, width), BF16),
            pltpu.VMEM((width, heads * DH), BF16),
            pltpu.VMEM((width, heads * DH), BF16),
            pltpu.VMEM((width, heads * DH), BF16),
            pltpu.VMEM((32, width), BF16),
            pltpu.VMEM((1, 16), F32),
            pltpu.VMEM((TP, seqs, width // TP), BF16),
            pltpu.VMEM((rows, heads * DH), BF16),
            pltpu.VMEM((rows, heads * DH), BF16),
            pltpu.VMEM((rows, 128), F32),
            pltpu.VMEM((span, span), BF16),
            pltpu.VMEM((2 * 16, span), F32),
            pltpu.VMEM((2, 2 * 16, 128), F32),
            pltpu.VMEM((SP // 2, 2, MSG, 128), BF16),
            pltpu.VMEM((SP, MSG, 128), BF16),
            pltpu.VMEM((2, 128), F32),
            pltpu.VMEM((SP, 2, 128), F32),
            dma((5,)),
            dma((len(BLOCKS),)),
            dma((CHUNKS, 2)),
            dma((2,)),
            dma((2,)),
            dma((2,)),
        ],
        compiler_params=pltpu.CompilerParams(
            collective_id=0, has_side_effects=True, vmem_limit_bytes=60 * 1024 * 1024
        ),
    )(
        inputs.reshape(rows, width), w_key, w_value, w_query,
        w_igate.T, w_fgate.T, forget_bias.reshape(1, -1), new_rows,
    )
    return pl.pallas_call(unpack, out_shape=out_shape, in_specs=[vmem], out_specs=[vmem] * 4)(
        pltpu.with_memory_space_constraint(packed, pltpu.VMEM)
    )


def solution(mesh):
    in_specs = (
        P(None, "sp", None),
        P(None, "tp"),
        P(None, "tp"),
        P(None, "tp"),
        P(),
        P(),
        P(),
        P(None, "tp"),
    )
    out_specs = (P(None, "tp", "sp", None), P(None, "tp", "sp"), P(None, "tp"), P(None, "tp", "sp"))
    return jax.shard_map(shards, mesh=mesh, in_specs=in_specs, out_specs=out_specs, check_vma=False)
```

```python
import functools

import jax
import jax.numpy as jnp
from jax import lax
from jax.experimental import pallas as pl
from jax.experimental.pallas import tpu as pltpu
from jax.sharding import PartitionSpec as P

DH = 128
EPS = 1e-06
MESH = pl.DeviceIdType.MESH
F32 = jnp.float32
BF16 = jnp.bfloat16
NZ, NY = 8, 4
SP, TP = NZ * NY, 8
ROWS = 128
TILE = 256
MSG = 8


def peer_offsets():
    offsets = [(dz, dy) for dz in range(NZ) for dy in range(NY) if dz or dy]
    return sorted(offsets, key=lambda o: -(min(o[0], NZ - o[0]) + min(o[1], NY - o[1])))


def iota(shape, dim):
    return lax.broadcasted_iota(jnp.int32, shape, dim)


def log_sigmoid(v):
    u = jnp.exp(-jnp.abs(v))
    series = u * (1.0 - u * (0.5 - u * (1.0 / 3.0 - u * (0.25 - u * (0.2 - u * (1.0 / 6.0))))))
    return jnp.minimum(v, 0.0) - jnp.where(u < 0.03, series, jnp.log(1.0 + u))


def split3(v):
    hi = v.astype(BF16).astype(F32)
    rest = v - hi
    mid = rest.astype(BF16).astype(F32)
    return hi, mid, rest - mid


def kernel(
    x_hbm, wk_hbm, wv_hbm, wq_hbm, wi_hbm, wf_hbm, bias_hbm, new_hbm,
    packed_out,
    x, xn, wk, wv, wq, wg, bias, fresh, acc_g, tri, wrow, stat,
    send_m, recv_m, send_n, recv_n, send_s, recv_s,
    load_sem, x_sem, w_sem, new_sem, msem, nsem, ssem,
):
    sp, tp = lax.axis_index("sp"), lax.axis_index("tp")
    z, y = sp // NY, lax.rem(sp, NY)
    span, width = xn[0].shape
    per_seq = span // ROWS
    peers = []
    for dz, dy in peer_offsets():
        peers.append(lax.rem(z + dz, NZ) * NY + lax.rem(y + dy, NY))
    tp_peers = [lax.rem(tp + k, TP) for k in range(1, TP)]

    def load(hbm, vmem, sem, parts):
        each = vmem.shape[0] // parts
        copies = []
        for i in range(parts):
            part = pl.ds(i * each, each)
            copies.append(pltpu.make_async_copy(hbm.at[part], vmem.at[part], sem))
        return copies, pltpu.make_async_copy(hbm, vmem, sem)

    def start(*loads):
        for copies, _ in loads:
            for copy in copies:
                copy.start()

    def land(*loads):
        for _, whole in loads:
            whole.wait()

    small = [
        load(wi_hbm, wg.at[pl.ds(0, 16)], load_sem.at[0], 1),
        load(wf_hbm, wg.at[pl.ds(16, 16)], load_sem.at[1], 1),
        load(bias_hbm, bias, load_sem.at[2], 1),
        load(new_hbm, fresh.at[tp], load_sem.at[3], 1),
    ]
    x_loads = [
        load(x_hbm.at[pl.ds(i * ROWS, ROWS)], x[i], x_sem.at[i], 8) for i in range(2 * per_seq)
    ]
    half = width // 2
    w_loads = []
    for i in range(2):
        part = pl.ds(i * half, half)
        w_loads.append(load(wv_hbm.at[part], wv.at[part], w_sem.at[0, i], 4))
        w_loads.append(load(wk_hbm.at[part], wk.at[part], w_sem.at[1, i], 4))
    load_q = load(wq_hbm, wq, load_sem.at[4], 4)
    start(x_loads[0], *small)

    barrier = pltpu.get_barrier_semaphore()
    for p in peers:
        pl.semaphore_signal(barrier, inc=1, device_id=(p, tp), device_id_type=MESH)
    for p in tp_peers:
        pl.semaphore_signal(barrier, inc=1, device_id=(sp, p), device_id_type=MESH)
    start(*x_loads[1:3])
    tri[...] = (iota((span, span), 0) > iota((span, span), 1)).astype(F32).astype(BF16)

    def root(i, top, count):
        total = None
        for c in range(0, width, 128):
            piece = x[i][top:top + count, c:c + 128].astype(F32)
            total = piece * piece if total is None else total + piece * piece
        mean = jnp.sum(total, axis=1, keepdims=True) * (1.0 / width)
        return lax.rsqrt(mean + EPS), total

    def gate(blocks, roots):
        totals = {}
        for c in range(0, width, TILE):
            for i in blocks:
                s, at = i // per_seq, (i % per_seq) * ROWS
                normed = (x[i][:, c:c + TILE].astype(F32) * roots[i]).astype(BF16)
                xn[s][at:at + ROWS, c:c + TILE] = normed
                for half_of in range(2):
                    top = half_of * ROWS // 2
                    part = lax.dot_general(
                        normed[top:top + ROWS // 2], wg[:, c:c + TILE],
                        (((1,), (1,)), ((), ())), preferred_element_type=F32,
                    )
                    key = i, half_of
                    totals[key] = part if key not in totals else totals[key] + part
        for (i, half_of), total in totals.items():
            s, at = i // per_seq, (i % per_seq) * ROWS + half_of * ROWS // 2
            acc_g[s][at:at + ROWS // 2, 0:32] = total

    def project(s, sums, tiles, between=None):
        for t in tiles:
            rows_n = xn[s][:, t * TILE:(t + 1) * TILE]
            zero = between[t]() if between and t in between else None
            if zero is not None:
                rows_n = jnp.concatenate([rows_n[0:16] + zero, rows_n[16:]], axis=0)
            for j, w in enumerate((wv, wk)):
                part = jnp.dot(rows_n, w[t * TILE:(t + 1) * TILE, :], preferred_element_type=F32)
                sums[j] = part if sums[j] is None else sums[j] + part

    eye = iota((16, 128), 0) == iota((16, 128), 1)

    def gates(s):
        bias_col = jnp.sum(jnp.where(eye, bias_row, 0.0), axis=1, keepdims=True)
        turned = acc_g[s][...].T
        logf = log_sigmoid(turned[16:32] + bias_col)
        lhs = jnp.concatenate(split3(logf), axis=0).astype(BF16)
        after = jnp.dot(lhs, tri[...], preferred_element_type=F32)
        rest = after[0:16] + after[16:32] + after[32:48]
        logw = rest + turned[0:16]
        top = jnp.max(logw, axis=1, keepdims=True)
        wrow[pl.ds(16 * s, 16), :] = jnp.exp(logw - top)
        stat[0, pl.ds(16 * s, 16), :] = jnp.broadcast_to(rest[:, 0:1] + logf[:, 0:1], (16, 128))
        stat[1, pl.ds(16 * s, 16), :] = jnp.broadcast_to(top, (16, 128))

    def memory(s, value, key):
        mats, nrms = [], []
        for h in range(2):
            w = wrow[pl.ds(16 * s + 2 * tp + h, 1), :]
            cols = slice(h * DH, (h + 1) * DH)
            turned = (value[:, cols].T.astype(F32) * w).astype(BF16)
            hi, mid, low = split3(w)
            row = iota((16, span), 0)
            extra = jnp.where(row == 0, hi, jnp.where(row == 1, mid, jnp.where(row == 2, low, 0.0)))
            out = jnp.dot(
                jnp.concatenate([turned, extra.astype(BF16)], axis=0),
                key[:, cols],
                preferred_element_type=F32,
            )
            mats.append(out[0:128].reshape(16, 8, 128))
            nrms.append(out[128:129] + out[129:130] + out[130:131])
        low_half = iota((16, 8, 128), 1) < 4
        a, b = mats
        send_m[s][:, 0] = jnp.where(low_half, a, pltpu.roll(b, 4, 1)).astype(BF16)
        send_m[s][:, 1] = jnp.where(low_half, pltpu.roll(a, 4, 1), b).astype(BF16)
        send_n[s][...] = jnp.concatenate(nrms, axis=0)

    def send_memory(s):
        for p in peers:
            pltpu.make_async_remote_copy(
                src_ref=send_m[s].at[p // 2, lax.rem(p, 2)], dst_ref=recv_m[s].at[sp],
                send_sem=msem.at[s, 0], recv_sem=msem.at[s, 1],
                device_id=(p, tp), device_id_type=MESH,
            ).start()
            pltpu.make_async_remote_copy(
                src_ref=send_n[s], dst_ref=recv_n[s].at[sp],
                send_sem=nsem.at[s, 0], recv_sem=nsem.at[s, 1],
                device_id=(p, tp), device_id_type=MESH,
            ).start()
        recv_m[s][sp] = send_m[s][sp // 2, lax.rem(sp, 2)]
        recv_n[s][sp] = send_n[s][...]

    roots = {}
    for i in range(per_seq):
        land(x_loads[i])
        if i == 0:
            start(w_loads[0], w_loads[1])
        else:
            start(*((w_loads[2], w_loads[3]) if i == 1 else x_loads[per_seq:]))
        roots[i] = root(i, 0, ROWS)[0]
    land(*small)
    bias_row = jnp.concatenate([bias[...], jnp.zeros((1, 112), F32)], axis=1)
    gate(range(per_seq), roots)

    tiles = width // TILE
    land(*w_loads[:2])
    start(load_q)
    sums_a, sums_b = [None, None], [None, None]
    project(0, sums_a, range(tiles // 2))
    land(*w_loads[2:], *x_loads[per_seq:])
    groups = [(i, top) for i in range(per_seq, 2 * per_seq) for top in range(0, ROWS, 16)]
    found = {}

    def squares(t):
        share = len(groups) // (tiles // 2)
        zero = None
        for i, top in groups[(t - tiles // 2) * share:(t - tiles // 2 + 1) * share]:
            found[i, top], total = root(i, top, 16)
            low = jnp.minimum(total, 0.0)
            zero = low if zero is None else zero + low
        return jnp.concatenate([zero, zero], axis=1).astype(BF16)

    def with_gates(t):
        gates(0)
        return squares(t)

    between = {t: functools.partial(squares, t) for t in range(tiles // 2, tiles)}
    between[tiles - 4] = functools.partial(with_gates, tiles - 4)
    project(0, sums_a, range(tiles // 2, tiles), between)
    for i in range(per_seq, 2 * per_seq):
        roots[i] = jnp.concatenate([found[i, top] for top in range(0, ROWS, 16)], axis=0)
    value_a, key_a = (total.astype(BF16) for total in sums_a)
    gate(range(per_seq, 2 * per_seq), roots)

    def scalars():
        gates(1)
        lane = iota((1, 128), 1)
        line = jnp.zeros((1, 128), F32)
        for i in range(2):
            for q in range(4):
                own = stat[i, pl.ds(16 * (q // 2) + 2 * tp + q % 2, 1), :]
                line = jnp.where((lane >= 64 * i + 4 * q) & (lane < 64 * i + 4 * q + 4), own, line)
        send_s[...] = line
        recv_s[sp] = line

    def send_scalars():
        for p in peers:
            pltpu.make_async_remote_copy(
                src_ref=send_s, dst_ref=recv_s.at[sp], send_sem=ssem.at[0], recv_sem=ssem.at[1],
                device_id=(p, tp), device_id_type=MESH,
            ).start()

    def send_token():
        for p in tp_peers:
            pltpu.make_async_remote_copy(
                src_ref=fresh.at[tp], dst_ref=fresh.at[tp], send_sem=new_sem.at[0], recv_sem=new_sem.at[1],
                device_id=(sp, p), device_id_type=MESH,
            ).start()

    pl.semaphore_wait(barrier, SP - 1 + TP - 1)
    between = {
        2: lambda: memory(0, value_a, key_a), 6: lambda: send_memory(0), 7: scalars, 11: send_scalars,
    }
    project(1, sums_b, range(tiles), between)
    value_b, key_b = (total.astype(BF16) for total in sums_b)
    memory(1, value_b, key_b)
    send_memory(1)
    send_token()

    got = fresh.at[pl.ds(0, TP - 1)]
    pltpu.make_async_copy(got, got, new_sem.at[1]).wait()
    pieces = [fresh[k].astype(F32) for k in range(TP)]
    fresh_row = jnp.concatenate(pieces, axis=1)
    mean = jnp.sum(fresh_row * fresh_row, axis=1, keepdims=True) * (1.0 / width)
    token = (fresh_row * lax.rsqrt(mean + EPS)).astype(BF16)
    land(load_q)
    key = jnp.dot(token, wk[...], preferred_element_type=F32).astype(BF16).astype(F32)
    value = jnp.dot(token, wv[...], preferred_element_type=F32).astype(BF16).astype(F32)
    query = jnp.dot(token, wq[...], preferred_element_type=F32).astype(BF16).astype(F32)
    new_gate = lax.dot_general(token, wg[...], (((1,), (1,)), ((), ())), preferred_element_type=F32)

    def per_row(v, s):
        return jnp.concatenate(
            [jnp.broadcast_to(v[s:s + 1, h * DH:(h + 1) * DH], (4, DH)) for h in range(2)], axis=0
        )

    def picked(v, at):
        return jnp.sum(jnp.where(iota((8, v.shape[1]), 1) == at, v, 0.0), axis=1, keepdims=True)

    row8 = iota((8, 1), 0)
    own_row = 4 * sp + lax.rem(row8, 4)
    head = 2 * tp + row8 // 4
    bias_own = picked(jnp.broadcast_to(bias_row, (8, 128)), head)
    fresh_terms = []
    for s in range(2):
        q_rows, k_rows, v_rows = (per_row(v, s) for v in (query, key, value))
        agreement = jnp.sum(q_rows * k_rows, axis=1, keepdims=True)
        value_own = picked(v_rows, own_row)
        gate_rows = jnp.broadcast_to(new_gate[s:s + 1], (8, 32))
        input_new = picked(gate_rows, head)
        forget_new = log_sigmoid(picked(gate_rows, 16 + head) + bias_own)
        fresh_terms.append((q_rows, agreement, value_own, input_new, forget_new))

    got = recv_s.at[pl.ds(0, SP - 1)]
    pltpu.make_async_copy(got, got, ssem.at[1]).wait()
    arrived = recv_s[:, 0, :]
    later = (iota((SP, SP), 1) > iota((SP, SP), 0)).astype(F32).astype(BF16)
    sums = jnp.dot(later, jnp.concatenate(split3(arrived), axis=1).astype(BF16), preferred_element_type=F32)
    lw = sums[:, 0:128] + sums[:, 128:256] + sums[:, 256:384] + pltpu.roll(arrived, 64, 1)
    top = jnp.max(lw, axis=0, keepdims=True)
    scale = jnp.exp(lw - top)
    stacked = jnp.concatenate([scale, jnp.broadcast_to(top, (8, 128)), jnp.zeros((88, 128), F32)], axis=0)
    turned = stacked.T

    factor = DH ** (-0.5)
    lane8 = iota((8, 128), 1)
    table = []
    for s in range(2):
        q_rows, agreement, value_own, input_new, forget_new = fresh_terms[s]
        top_col = turned[8 * s:8 * s + 8, SP:SP + 1]
        share = turned[8 * s:8 * s + 8, 0:SP]
        top_next = jnp.maximum(forget_new + top_col, input_new)
        old_share = jnp.exp(forget_new + top_col - top_next)
        new_share = jnp.exp(input_new - top_next)
        got = recv_m[s].at[pl.ds(0, SP - 1)]
        pltpu.make_async_copy(got, got, msem.at[s, 1]).wait()
        got = recv_n[s].at[pl.ds(0, SP - 1)]
        pltpu.make_async_copy(got, got, nsem.at[s, 1]).wait()
        merged = [jnp.zeros((8, 128), F32) for _ in range(4)]
        for d in range(SP):
            merged[d % 4] = merged[d % 4] + share[:, d:d + 1] * recv_m[s][d].astype(F32)
        merged = (merged[0] + merged[1]) + (merged[2] + merged[3])
        matrix = merged.astype(BF16)
        n_rows = []
        for h in range(2):
            at = 8 * s + 4 * h
            normal = jnp.sum(scale[:, at:at + 1] * recv_n[s][:, h, :], axis=0, keepdims=True)
            n_rows.append(jnp.broadcast_to(normal, (4, 128)))
        n_rows = jnp.concatenate(n_rows, axis=0)
        numer = jnp.sum(matrix.astype(F32) * q_rows, axis=1, keepdims=True)
        numer = (old_share * numer + new_share * agreement * value_own) * factor
        denom = jnp.sum(n_rows * q_rows, axis=1, keepdims=True)
        denom = (old_share * denom + new_share * agreement) * factor
        read = numer / jnp.maximum(jnp.abs(denom), 1.0)
        own_normal = picked(n_rows, own_row)
        table.append(jnp.where(lane8 == 0, own_normal, jnp.where(lane8 == 1, top_col, read)))
        packed_out[8 * s:8 * s + 8] = merged
    packed_out[16:24] = jnp.concatenate([*table, jnp.zeros((112, 128), F32)], axis=0).T[0:8]

    sent = recv_s.at[pl.ds(0, SP - 1)]
    pltpu.make_async_copy(sent, sent, ssem.at[0]).wait()
    for s in range(2):
        sent = recv_m[s].at[pl.ds(0, SP - 1)]
        pltpu.make_async_copy(sent, sent, msem.at[s, 0]).wait()
        sent = recv_n[s].at[pl.ds(0, SP - 1)]
        pltpu.make_async_copy(sent, sent, nsem.at[s, 0]).wait()
    sent = fresh.at[pl.ds(0, TP - 1)]
    pltpu.make_async_copy(sent, sent, new_sem.at[0]).wait()


def unpack(packed, mat_out, nrm_out, top_out, read_out):
    for q in range(4):
        s, h = q // 2, q % 2
        lanes = slice(4 * q, 4 * q + 4)
        mat_out[s, h] = packed[lanes].astype(BF16)
        nrm_out[s, h:h + 1, :] = packed[16:17, lanes]
        top_out[s:s + 1, h:h + 1] = packed[17:18, 4 * q:4 * q + 1]
        read_out[s, h:h + 1, :] = packed[18:19, lanes].astype(BF16)


def shards(inputs, w_key, w_value, w_query, w_igate, w_fgate, forget_bias, new_rows):
    seqs, span, width = inputs.shape
    rows = seqs * span
    heads = w_key.shape[1] // DH
    out_shape = (
        jax.ShapeDtypeStruct((seqs, heads, DH // SP, DH), BF16),
        jax.ShapeDtypeStruct((seqs, heads, DH // SP), F32),
        jax.ShapeDtypeStruct((seqs, heads), F32),
        jax.ShapeDtypeStruct((seqs, heads, DH // SP), BF16),
    )
    hbm = pl.BlockSpec(memory_space=pl.ANY)
    vmem = pl.BlockSpec(memory_space=pltpu.VMEM)
    dma = pltpu.SemaphoreType.DMA
    packed = pl.pallas_call(
        kernel,
        out_shape=pltpu.VMEM((24, 128), F32),
        in_specs=[hbm] * 8,
        out_specs=vmem,
        scratch_shapes=[
            [pltpu.VMEM((ROWS, width), BF16) for _ in range(rows // ROWS)],
            [pltpu.VMEM((span, width), BF16) for _ in range(seqs)],
            pltpu.VMEM((width, heads * DH), BF16),
            pltpu.VMEM((width, heads * DH), BF16),
            pltpu.VMEM((width, heads * DH), BF16),
            pltpu.VMEM((32, width), BF16),
            pltpu.VMEM((1, 16), F32),
            pltpu.VMEM((TP, seqs, width // TP), BF16),
            [pltpu.VMEM((span, 128), F32) for _ in range(seqs)],
            pltpu.VMEM((span, span), BF16),
            pltpu.VMEM((2 * 16, span), F32),
            pltpu.VMEM((2, 2 * 16, 128), F32),
            [pltpu.VMEM((SP // 2, 2, MSG, 128), BF16) for _ in range(seqs)],
            [pltpu.VMEM((SP, MSG, 128), BF16) for _ in range(seqs)],
            [pltpu.VMEM((2, 128), F32) for _ in range(seqs)],
            [pltpu.VMEM((SP, 2, 128), F32) for _ in range(seqs)],
            pltpu.VMEM((1, 128), F32),
            pltpu.VMEM((SP, 1, 128), F32),
            dma((5,)),
            dma((rows // ROWS,)),
            dma((2, 2)),
            dma((2,)),
            dma((seqs, 2)),
            dma((seqs, 2)),
            dma((2,)),
        ],
        compiler_params=pltpu.CompilerParams(
            collective_id=0, has_side_effects=True, vmem_limit_bytes=60 * 1024 * 1024
        ),
    )(
        inputs.reshape(rows, width), w_key, w_value, w_query,
        w_igate.T, w_fgate.T, forget_bias.reshape(1, -1), new_rows,
    )
    return pl.pallas_call(unpack, out_shape=out_shape, in_specs=[vmem], out_specs=[vmem] * 4)(
        pltpu.with_memory_space_constraint(packed, pltpu.VMEM)
    )


def solution(mesh):
    in_specs = (
        P(None, "sp", None),
        P(None, "tp"),
        P(None, "tp"),
        P(None, "tp"),
        P(),
        P(),
        P(),
        P(None, "tp"),
    )
    out_specs = (P(None, "tp", "sp", None), P(None, "tp", "sp"), P(None, "tp"), P(None, "tp", "sp"))
    return jax.shard_map(shards, mesh=mesh, in_specs=in_specs, out_specs=out_specs, check_vma=False)
```

```python
import functools

import jax
import jax.numpy as jnp
from jax import lax
from jax.experimental import pallas as pl
from jax.experimental.pallas import tpu as pltpu
from jax.sharding import PartitionSpec as P

DH = 128
EPS = 1e-06
MESH = pl.DeviceIdType.MESH
F32 = jnp.float32
BF16 = jnp.bfloat16
NZ, NY = 8, 4
SP, TP = NZ * NY, 8
ROWS = 128
TILE = 256
MSG = 8


def peer_offsets():
    offsets = [(dz, dy) for dz in range(NZ) for dy in range(NY) if dz or dy]
    return sorted(offsets, key=lambda o: -(min(o[0], NZ - o[0]) + min(o[1], NY - o[1])))


def iota(shape, dim):
    return lax.broadcasted_iota(jnp.int32, shape, dim)


def log_sigmoid(v):
    u = jnp.exp(-jnp.abs(v))
    series = u * (1.0 - u * (0.5 - u * (1.0 / 3.0 - u * (0.25 - u * (0.2 - u * (1.0 / 6.0))))))
    return jnp.minimum(v, 0.0) - jnp.where(u < 0.03, series, jnp.log(1.0 + u))


def split3(v):
    hi = v.astype(BF16).astype(F32)
    rest = v - hi
    mid = rest.astype(BF16).astype(F32)
    return hi, mid, rest - mid


def kernel(
    x_hbm, wk_hbm, wv_hbm, wq_hbm, wi_hbm, wf_hbm, bias_hbm, new_hbm,
    packed_out,
    x, xn, w_vk, wq, wg, bias, fresh, acc_g, tri, wrow, stat,
    send_m, recv_m, send_n, recv_n, send_s, recv_s,
    sems, new_sem, msem, nsem, ssem,
):
    sp, tp = lax.axis_index("sp"), lax.axis_index("tp")
    z, y = sp // NY, lax.rem(sp, NY)
    span, width = xn[0].shape
    per_seq = span // ROWS
    peers = []
    for dz, dy in peer_offsets():
        peers.append(lax.rem(z + dz, NZ) * NY + lax.rem(y + dy, NY))
    tp_peers = [lax.rem(tp + k, TP) for k in range(1, TP)]

    def load(hbm, vmem, sem, parts):
        each = vmem.shape[0] // parts
        copies = []
        for i in range(parts):
            part = pl.ds(i * each, each)
            copies.append(pltpu.make_async_copy(hbm.at[part], vmem.at[part], sem))
        return copies, pltpu.make_async_copy(hbm, vmem, sem)

    def start(*loads):
        for copies, _ in loads:
            for copy in copies:
                copy.start()

    def land(*loads):
        for _, whole in loads:
            whole.wait()

    gate_load = (
        [
            pltpu.make_async_copy(wi_hbm, wg.at[pl.ds(0, 16)], sems.at[6]),
            pltpu.make_async_copy(wf_hbm, wg.at[pl.ds(16, 16)], sems.at[6]),
        ],
        pltpu.make_async_copy(wg, wg, sems.at[6]),
    )
    small = [load(bias_hbm, bias, sems.at[7], 1), load(new_hbm, fresh.at[tp], sems.at[8], 1)]
    x_loads = [
        load(x_hbm.at[pl.ds(i * ROWS, ROWS)], x[i], sems.at[i], 8) for i in range(2 * per_seq)
    ]
    half = width // 2
    w_loads = []
    for i in range(2):
        part, w_sem = pl.ds(i * half, half), sems.at[(9, 1)[i]]
        copies = []
        for j, hbm in enumerate((wv_hbm, wk_hbm)):
            copies += load(hbm.at[part], w_vk.at[j, part], w_sem, 4)[0]
        w_loads.append((copies, pltpu.make_async_copy(w_vk.at[:, part], w_vk.at[:, part], w_sem)))
    load_q = load(wq_hbm, wq, sems.at[2], 4)
    start(gate_load, x_loads[0], *small)

    barrier = pltpu.get_barrier_semaphore()
    for p in peers:
        pl.semaphore_signal(barrier, inc=1, device_id=(p, tp), device_id_type=MESH)
    for p in tp_peers:
        pl.semaphore_signal(barrier, inc=1, device_id=(sp, p), device_id_type=MESH)
    start(*x_loads[1:3])
    tri[...] = (iota((span, span), 0) > iota((span, span), 1)).astype(F32).astype(BF16)
    start(w_loads[0])

    def root(i, top, count):
        total = None
        for c in range(0, width, 128):
            piece = x[i][top:top + count, c:c + 128].astype(F32)
            total = piece * piece if total is None else total + piece * piece
        mean = jnp.sum(total, axis=1, keepdims=True) * (1.0 / width)
        return lax.rsqrt(mean + EPS), total

    def gate(blocks, roots, squares=None, between=None):
        totals = {}
        for t in range(width // TILE):
            c = t * TILE
            if between and t in between:
                between[t]()
            for i in blocks:
                s, at = i // per_seq, (i % per_seq) * ROWS
                normed = (x[i][:, c:c + TILE].astype(F32) * roots[i]).astype(BF16)
                xn[s][at:at + ROWS, c:c + TILE] = normed
                zero = squares(t) if squares else None
                if zero is not None:
                    normed = jnp.concatenate([normed[0:16] + zero, normed[16:]], axis=0)
                for half_of in range(2):
                    top = half_of * ROWS // 2
                    part = lax.dot_general(
                        normed[top:top + ROWS // 2], wg[:, c:c + TILE],
                        (((1,), (1,)), ((), ())), preferred_element_type=F32,
                    )
                    key = i, half_of
                    totals[key] = part if key not in totals else totals[key] + part
        for (i, half_of), total in totals.items():
            s, at = i // per_seq, (i % per_seq) * ROWS + half_of * ROWS // 2
            acc_g[s][at:at + ROWS // 2, 0:32] = total

    def squares_of(found, blocks, first, count, stride=1):
        groups = [(i, top) for i in blocks for top in range(0, ROWS, 16)]
        share = len(groups) // count

        def squares(t):
            at, odd = divmod(t - first, stride)
            if odd or not 0 <= at < count:
                return None
            zero = None
            for i, top in groups[at * share:(at + 1) * share]:
                found[i, top], total = root(i, top, 16)
                low = jnp.minimum(total, 0.0)
                zero = low if zero is None else zero + low
            return jnp.concatenate([zero, zero], axis=1).astype(BF16)

        return squares

    def project(s, sums, tiles, squares=None, between=None):
        for t in tiles:
            if between and t in between:
                between[t]()
            rows_n = xn[s][:, t * TILE:(t + 1) * TILE]
            zero = squares(t) if squares else None
            if zero is not None:
                rows_n = jnp.concatenate([rows_n[0:16] + zero, rows_n[16:]], axis=0)
            for j in range(2):
                part = jnp.dot(rows_n, w_vk[j, t * TILE:(t + 1) * TILE, :], preferred_element_type=F32)
                sums[j] = part if sums[j] is None else sums[j] + part

    eye = iota((16, 128), 0) == iota((16, 128), 1)

    def gates(s):
        bias_col = jnp.sum(jnp.where(eye, bias_row, 0.0), axis=1, keepdims=True)
        turned = acc_g[s][...].T
        logf = log_sigmoid(turned[16:32] + bias_col)
        lhs = jnp.concatenate(split3(logf), axis=0).astype(BF16)
        after = jnp.dot(lhs, tri[...], preferred_element_type=F32)
        rest = after[0:16] + after[16:32] + after[32:48]
        logw = rest + turned[0:16]
        top = jnp.max(logw, axis=1, keepdims=True)
        wrow[pl.ds(16 * s, 16), :] = jnp.exp(logw - top)
        stat[0, pl.ds(16 * s, 16), :] = jnp.broadcast_to(rest[:, 0:1] + logf[:, 0:1], (16, 128))
        stat[1, pl.ds(16 * s, 16), :] = jnp.broadcast_to(top, (16, 128))

    def own_weight(s, h):
        return wrow[pl.ds(16 * s + 2 * tp + h, 1), :]

    def normalizer(s, key):
        row = iota((16, span), 0)
        lhs = jnp.zeros((16, span), F32)
        for h in range(2):
            for i, part in enumerate(split3(own_weight(s, h))):
                lhs = jnp.where(row == 3 * h + i, part, lhs)
        out = jnp.dot(lhs.astype(BF16), key, preferred_element_type=F32)
        send_n[s][...] = jnp.concatenate(
            [out[0:1, 0:DH] + out[1:2, 0:DH] + out[2:3, 0:DH], out[3:4, DH:] + out[4:5, DH:] + out[5:6, DH:]], axis=0
        )

    def memory(s, value, key):
        mats = []
        for h in range(2):
            cols = slice(h * DH, (h + 1) * DH)
            turned = (value[:, cols].T.astype(F32) * own_weight(s, h)).astype(BF16)
            out = jnp.dot(turned, key[:, cols], preferred_element_type=F32)
            mats.append(out.reshape(16, 8, 128))
        low_half = iota((16, 8, 128), 1) < 4
        a, b = mats
        send_m[s][:, 0] = jnp.where(low_half, a, pltpu.roll(b, 4, 1)).astype(BF16)
        send_m[s][:, 1] = jnp.where(low_half, pltpu.roll(a, 4, 1), b).astype(BF16)

    def send_memory(s):
        for p in peers:
            pltpu.make_async_remote_copy(
                src_ref=send_m[s].at[p // 2, lax.rem(p, 2)], dst_ref=recv_m[s].at[sp],
                send_sem=sems.at[3 + s], recv_sem=msem.at[s],
                device_id=(p, tp), device_id_type=MESH,
            ).start()
            pltpu.make_async_remote_copy(
                src_ref=send_n[s], dst_ref=recv_n[s].at[sp],
                send_sem=sems.at[5 + s], recv_sem=nsem.at[s],
                device_id=(p, tp), device_id_type=MESH,
            ).start()
        recv_m[s][sp] = send_m[s][sp // 2, lax.rem(sp, 2)]
        recv_n[s][sp] = send_n[s][...]

    tiles = width // TILE
    roots, found = {}, {}

    def collected(i):
        roots[i] = jnp.concatenate([found[i, top] for top in range(0, ROWS, 16)], axis=0)

    land(x_loads[0])
    start(*x_loads[3:5])
    roots[0] = root(0, 0, ROWS)[0]
    land(gate_load, x_loads[1], *small)
    start(w_loads[1], x_loads[5])
    bias_row = jnp.concatenate([bias[...], jnp.zeros((1, 112), F32)], axis=1)
    gate([0], roots, squares_of(found, [1], 0, 8, 2))
    collected(1)
    land(x_loads[2])
    gate([1], roots, squares_of(found, [2], 0, 8, 2))
    collected(2)
    gate([2], roots)

    land(w_loads[0], *x_loads[3:5])
    start(load_q)
    sums_a, sums_b = [None, None], [None, None]
    project(0, sums_a, range(tiles // 2), squares_of(found, [3, 4], 0, 8))
    land(w_loads[1], x_loads[5])
    pl.semaphore_wait(barrier, SP - 1 + TP - 1)
    project(0, sums_a, range(tiles // 2, tiles), squares_of(found, [5], tiles // 2, 8))
    for i in range(per_seq, 2 * per_seq):
        collected(i)
    value_a, key_a = (total.astype(BF16) for total in sums_a)
    def first_memory():
        memory(0, value_a, key_a)
        normalizer(0, key_a)

    gate(range(per_seq, 2 * per_seq), roots, None, {8: lambda: gates(0)})

    def scalars():
        lane = iota((1, 128), 1)
        line = jnp.zeros((1, 128), F32)
        for i in range(2):
            for q in range(4):
                own = stat[i, pl.ds(16 * (q // 2) + 2 * tp + q % 2, 1), :]
                line = jnp.where((lane >= 64 * i + 4 * q) & (lane < 64 * i + 4 * q + 4), own, line)
        send_s[...] = line
        recv_s[sp] = line

    def send_scalars():
        for p in peers:
            pltpu.make_async_remote_copy(
                src_ref=send_s, dst_ref=recv_s.at[sp], send_sem=sems.at[7], recv_sem=ssem,
                device_id=(p, tp), device_id_type=MESH,
            ).start()

    def send_token():
        for p in tp_peers:
            pltpu.make_async_remote_copy(
                src_ref=fresh.at[tp], dst_ref=fresh.at[tp], send_sem=sems.at[8], recv_sem=new_sem,
                device_id=(sp, p), device_id_type=MESH,
            ).start()

    between = {
        1: send_token, 2: first_memory, 6: lambda: send_memory(0), 7: lambda: gates(1), 8: scalars, 11: send_scalars,
    }
    project(1, sums_b, range(tiles), None, between)
    value_b, key_b = (total.astype(BF16) for total in sums_b)
    normalizer(1, key_b)
    memory(1, value_b, key_b)
    send_memory(1)

    got = fresh.at[pl.ds(0, TP - 1)]
    pltpu.make_async_copy(got, got, sems.at[8]).wait()
    pltpu.make_async_copy(got, got, new_sem).wait()
    pieces = [fresh[k].astype(F32) for k in range(TP)]
    fresh_row = jnp.concatenate(pieces, axis=1)
    mean = jnp.sum(fresh_row * fresh_row, axis=1, keepdims=True) * (1.0 / width)
    token = (fresh_row * lax.rsqrt(mean + EPS)).astype(BF16)
    land(load_q)
    key = jnp.dot(token, w_vk[1], preferred_element_type=F32).astype(BF16).astype(F32)
    value = jnp.dot(token, w_vk[0], preferred_element_type=F32).astype(BF16).astype(F32)
    query = jnp.dot(token, wq[...], preferred_element_type=F32).astype(BF16).astype(F32)
    new_gate = lax.dot_general(token, wg[...], (((1,), (1,)), ((), ())), preferred_element_type=F32)

    def per_row(v, s):
        return jnp.concatenate(
            [jnp.broadcast_to(v[s:s + 1, h * DH:(h + 1) * DH], (4, DH)) for h in range(2)], axis=0
        )

    def picked(v, at):
        return jnp.sum(jnp.where(iota((8, v.shape[1]), 1) == at, v, 0.0), axis=1, keepdims=True)

    row8 = iota((8, 1), 0)
    own_row = 4 * sp + lax.rem(row8, 4)
    head = 2 * tp + row8 // 4
    bias_own = picked(jnp.broadcast_to(bias_row, (8, 128)), head)
    fresh_terms = []
    for s in range(2):
        q_rows, k_rows, v_rows = (per_row(v, s) for v in (query, key, value))
        agreement = jnp.sum(q_rows * k_rows, axis=1, keepdims=True)
        value_own = picked(v_rows, own_row)
        gate_rows = jnp.broadcast_to(new_gate[s:s + 1], (8, 32))
        input_new = picked(gate_rows, head)
        forget_new = log_sigmoid(picked(gate_rows, 16 + head) + bias_own)
        fresh_terms.append((q_rows, agreement, value_own, input_new, forget_new))

    got = recv_s.at[pl.ds(0, SP - 1)]
    pltpu.make_async_copy(got, got, sems.at[7]).wait()
    pltpu.make_async_copy(got, got, ssem).wait()
    arrived = recv_s[:, 0, :]
    later = (iota((SP, SP), 1) > iota((SP, SP), 0)).astype(F32).astype(BF16)
    sums = jnp.dot(later, jnp.concatenate(split3(arrived), axis=1).astype(BF16), preferred_element_type=F32)
    lw = sums[:, 0:128] + sums[:, 128:256] + sums[:, 256:384] + pltpu.roll(arrived, 64, 1)
    top = jnp.max(lw, axis=0, keepdims=True)
    scale = jnp.exp(lw - top)
    stacked = jnp.concatenate([scale, jnp.broadcast_to(top, (8, 128)), jnp.zeros((88, 128), F32)], axis=0)
    turned = stacked.T

    factor = DH ** (-0.5)
    lane8 = iota((8, 128), 1)
    table = []
    for s in range(2):
        q_rows, agreement, value_own, input_new, forget_new = fresh_terms[s]
        top_col = turned[8 * s:8 * s + 8, SP:SP + 1]
        share = turned[8 * s:8 * s + 8, 0:SP]
        top_next = jnp.maximum(forget_new + top_col, input_new)
        old_share = jnp.exp(forget_new + top_col - top_next)
        new_share = jnp.exp(input_new - top_next)
        shares = [jnp.broadcast_to(share[:, d:d + 1], (8, 128)) for d in range(SP)]
        scales = [jnp.broadcast_to(scale[:, 8 * s + 4 * h:8 * s + 4 * h + 1], (SP, 128)) for h in range(2)]
        got = recv_m[s].at[pl.ds(0, SP - 1)]
        pltpu.make_async_copy(got, got, sems.at[3 + s]).wait()
        pltpu.make_async_copy(got, got, msem.at[s]).wait()
        got = recv_n[s].at[pl.ds(0, SP - 1)]
        pltpu.make_async_copy(got, got, sems.at[5 + s]).wait()
        pltpu.make_async_copy(got, got, nsem.at[s]).wait()
        merged = [jnp.zeros((8, 128), F32) for _ in range(4)]
        for d in range(SP):
            merged[d % 4] = merged[d % 4] + shares[d] * recv_m[s][d].astype(F32)
        merged = (merged[0] + merged[1]) + (merged[2] + merged[3])
        matrix = merged.astype(BF16)
        n_rows = []
        for h in range(2):
            normal = jnp.sum(scales[h] * recv_n[s][:, h, :], axis=0, keepdims=True)
            n_rows.append(jnp.broadcast_to(normal, (4, 128)))
        n_rows = jnp.concatenate(n_rows, axis=0)
        numer = jnp.sum(matrix.astype(F32) * q_rows, axis=1, keepdims=True)
        numer = (old_share * numer + new_share * agreement * value_own) * factor
        denom = jnp.sum(n_rows * q_rows, axis=1, keepdims=True)
        denom = (old_share * denom + new_share * agreement) * factor
        read = numer / jnp.maximum(jnp.abs(denom), 1.0)
        own_normal = picked(n_rows, own_row)
        table.append(jnp.where(lane8 == 0, own_normal, jnp.where(lane8 == 1, top_col, read)))
        packed_out[8 * s:8 * s + 8] = merged
    packed_out[16:24] = jnp.concatenate([*table, jnp.zeros((112, 128), F32)], axis=0).T[0:8]


def unpack(packed, mat_out, nrm_out, top_out, read_out):
    for q in range(4):
        s, h = q // 2, q % 2
        lanes = slice(4 * q, 4 * q + 4)
        mat_out[s, h] = packed[lanes].astype(BF16)
        nrm_out[s, h:h + 1, :] = packed[16:17, lanes]
        top_out[s:s + 1, h:h + 1] = packed[17:18, 4 * q:4 * q + 1]
        read_out[s, h:h + 1, :] = packed[18:19, lanes].astype(BF16)


def shards(inputs, w_key, w_value, w_query, w_igate, w_fgate, forget_bias, new_rows):
    seqs, span, width = inputs.shape
    rows = seqs * span
    heads = w_key.shape[1] // DH
    out_shape = (
        jax.ShapeDtypeStruct((seqs, heads, DH // SP, DH), BF16),
        jax.ShapeDtypeStruct((seqs, heads, DH // SP), F32),
        jax.ShapeDtypeStruct((seqs, heads), F32),
        jax.ShapeDtypeStruct((seqs, heads, DH // SP), BF16),
    )
    hbm = pl.BlockSpec(memory_space=pl.ANY)
    vmem = pl.BlockSpec(memory_space=pltpu.VMEM)
    dma = pltpu.SemaphoreType.DMA
    packed = pl.pallas_call(
        kernel,
        out_shape=pltpu.VMEM((24, 128), F32),
        in_specs=[hbm] * 8,
        out_specs=vmem,
        scratch_shapes=[
            [pltpu.VMEM((ROWS, width), BF16) for _ in range(rows // ROWS)],
            [pltpu.VMEM((span, width), BF16) for _ in range(seqs)],
            pltpu.VMEM((2, width, heads * DH), BF16),
            pltpu.VMEM((width, heads * DH), BF16),
            pltpu.VMEM((32, width), BF16),
            pltpu.VMEM((1, 16), F32),
            pltpu.VMEM((TP, seqs, width // TP), BF16),
            [pltpu.VMEM((span, 128), F32) for _ in range(seqs)],
            pltpu.VMEM((span, span), BF16),
            pltpu.VMEM((2 * 16, span), F32),
            pltpu.VMEM((2, 2 * 16, 128), F32),
            [pltpu.VMEM((SP // 2, 2, MSG, 128), BF16) for _ in range(seqs)],
            [pltpu.VMEM((SP, MSG, 128), BF16) for _ in range(seqs)],
            [pltpu.VMEM((2, 128), F32) for _ in range(seqs)],
            [pltpu.VMEM((SP, 2, 128), F32) for _ in range(seqs)],
            pltpu.VMEM((1, 128), F32),
            pltpu.VMEM((SP, 1, 128), F32),
            dma((10,)),
            dma,
            dma((seqs,)),
            dma((seqs,)),
            dma,
        ],
        compiler_params=pltpu.CompilerParams(
            collective_id=0, has_side_effects=True, vmem_limit_bytes=60 * 1024 * 1024
        ),
    )(
        inputs.reshape(rows, width), w_key, w_value, w_query,
        w_igate.T, w_fgate.T, forget_bias.reshape(1, -1), new_rows,
    )
    return pl.pallas_call(unpack, out_shape=out_shape, in_specs=[vmem], out_specs=[vmem] * 4)(
        pltpu.with_memory_space_constraint(packed, pltpu.VMEM)
    )


def solution(mesh):
    in_specs = (
        P(None, "sp", None),
        P(None, "tp"),
        P(None, "tp"),
        P(None, "tp"),
        P(),
        P(),
        P(),
        P(None, "tp"),
    )
    out_specs = (P(None, "tp", "sp", None), P(None, "tp", "sp"), P(None, "tp"), P(None, "tp", "sp"))
    return jax.shard_map(shards, mesh=mesh, in_specs=in_specs, out_specs=out_specs, check_vma=False)
```

```python
import functools

import jax
import jax.numpy as jnp
from jax import lax
from jax.experimental import pallas as pl
from jax.experimental.pallas import tpu as pltpu
from jax.sharding import PartitionSpec as P

DH = 128
EPS = 1e-06
MESH = pl.DeviceIdType.MESH
F32 = jnp.float32
BF16 = jnp.bfloat16
NZ, NY = 8, 4
SP, TP = NZ * NY, 8
ROWS = 128
TILE = 256
MSG = 8


def peer_offsets():
    offsets = [(dz, dy) for dz in range(NZ) for dy in range(NY) if dz or dy]
    return sorted(offsets, key=lambda o: -(min(o[0], NZ - o[0]) + min(o[1], NY - o[1])))


def iota(shape, dim):
    return lax.broadcasted_iota(jnp.int32, shape, dim)


def log_sigmoid(v):
    u = jnp.exp(-jnp.abs(v))
    series = u * (1.0 - u * (0.5 - u * (1.0 / 3.0 - u * (0.25 - u * (0.2 - u * (1.0 / 6.0))))))
    return jnp.minimum(v, 0.0) - jnp.where(u < 0.03, series, jnp.log(1.0 + u))


def split3(v):
    hi = v.astype(BF16).astype(F32)
    rest = v - hi
    mid = rest.astype(BF16).astype(F32)
    return hi, mid, rest - mid


def kernel(
    x_hbm, wk_hbm, wv_hbm, wq_hbm, wi_hbm, wf_hbm, bias_hbm, new_hbm,
    packed_out,
    x, xn, w_vk, wq, wg, bias, fresh, acc_g, tri, wrow, mate_out, mate_in, table,
    send_m, recv_m, send_n, recv_n, send_s, recv_s,
    sems, mate_sem, new_sem, msem, nsem, ssem,
):
    sp, tp = lax.axis_index("sp"), lax.axis_index("tp")
    z, y = sp // NY, lax.rem(sp, NY)
    span, width = xn.shape
    per_seq = span // ROWS
    peers = []
    for dz, dy in peer_offsets():
        peers.append(lax.rem(z + dz, NZ) * NY + lax.rem(y + dy, NY))
    core = lax.rem(tp, 2)
    order = core, 1 - core
    mate = tp + 1 - 2 * core
    tp_peers = [lax.rem(tp + k, TP) for k in range(1, TP)]

    def load(hbm, vmem, sem, parts):
        each = vmem.shape[0] // parts
        copies = []
        for i in range(parts):
            part = pl.ds(i * each, each)
            copies.append(pltpu.make_async_copy(hbm.at[part], vmem.at[part], sem))
        return copies, pltpu.make_async_copy(hbm, vmem, sem)

    def start(*loads):
        for copies, _ in loads:
            for copy in copies:
                copy.start()

    def land(*loads):
        for _, whole in loads:
            whole.wait()

    gate_load = (
        [
            pltpu.make_async_copy(wi_hbm, wg.at[pl.ds(0, 16)], sems.at[6]),
            pltpu.make_async_copy(wf_hbm, wg.at[pl.ds(16, 16)], sems.at[6]),
        ],
        pltpu.make_async_copy(wg, wg, sems.at[6]),
    )
    small = [load(bias_hbm, bias, sems.at[7], 1), load(new_hbm, fresh.at[tp], sems.at[8], 1)]
    x_loads = [
        load(
            x_hbm.at[pl.ds(pl.multiple_of(order[i // per_seq] * span + i % per_seq * ROWS, ROWS), ROWS)],
            x[i], sems.at[i], 8,
        )
        for i in range(2 * per_seq)
    ]
    half = width // 2
    w_loads = []
    for i in range(2):
        part, w_sem = pl.ds(i * half, half), sems.at[(9, 1)[i]]
        copies = []
        for j, hbm in enumerate((wv_hbm, wk_hbm)):
            copies += load(hbm.at[part], w_vk.at[j, part], w_sem, 4)[0]
        w_loads.append((copies, pltpu.make_async_copy(w_vk.at[:, part], w_vk.at[:, part], w_sem)))
    load_q = load(wq_hbm, wq, sems.at[2], 4)
    start(gate_load, x_loads[0], *small)

    barrier = pltpu.get_barrier_semaphore()
    for p in peers:
        pl.semaphore_signal(barrier, inc=1, device_id=(p, tp), device_id_type=MESH)
    for p in tp_peers:
        pl.semaphore_signal(barrier, inc=1, device_id=(sp, p), device_id_type=MESH)
    start(*x_loads[1:3])
    tri[...] = (iota((span, span), 0) > iota((span, span), 1)).astype(F32).astype(BF16)
    start(w_loads[0])

    def root(i, top, count):
        total = None
        for c in range(0, width, 128):
            piece = x[i][top:top + count, c:c + 128].astype(F32)
            total = piece * piece if total is None else total + piece * piece
        mean = jnp.sum(total, axis=1, keepdims=True) * (1.0 / width)
        return lax.rsqrt(mean + EPS), total

    def gate(blocks, roots, squares=None, between=None):
        totals = {}
        for t in range(width // TILE):
            c = t * TILE
            if between and t in between:
                between[t]()
            for i in blocks:
                at = i * ROWS
                normed = (x[i][:, c:c + TILE].astype(F32) * roots[i]).astype(BF16)
                xn[at:at + ROWS, c:c + TILE] = normed
                zero = squares(t) if squares else None
                if zero is not None:
                    normed = jnp.concatenate([normed[0:16] + zero, normed[16:]], axis=0)
                for half_of in range(2):
                    top = half_of * ROWS // 2
                    part = lax.dot_general(
                        normed[top:top + ROWS // 2], wg[:, c:c + TILE],
                        (((1,), (1,)), ((), ())), preferred_element_type=F32,
                    )
                    key = i, half_of
                    totals[key] = part if key not in totals else totals[key] + part
        for (i, half_of), total in totals.items():
            at = i * ROWS + half_of * ROWS // 2
            acc_g[at:at + ROWS // 2, 0:32] = total

    def squares_of(found, blocks, first, count, stride=1):
        groups = [(i, top) for i in blocks for top in range(0, ROWS, 16)]
        share = len(groups) // count

        def squares(t):
            at, odd = divmod(t - first, stride)
            if odd or not 0 <= at < count:
                return None
            zero = None
            for i, top in groups[at * share:(at + 1) * share]:
                found[i, top], total = root(i, top, 16)
                low = jnp.minimum(total, 0.0)
                zero = low if zero is None else zero + low
            return jnp.concatenate([zero, zero], axis=1).astype(BF16)

        return squares

    def project(normed, sums, tiles, squares=None, between=None):
        for t in tiles:
            if between and t in between:
                between[t]()
            rows_n = normed(t)
            zero = squares(t) if squares else None
            if zero is not None:
                rows_n = jnp.concatenate([rows_n[0:16] + zero, rows_n[16:]], axis=0)
            for j in range(2):
                part = jnp.dot(rows_n, w_vk[j, t * TILE:(t + 1) * TILE, :], preferred_element_type=F32)
                sums[j] = part if sums[j] is None else sums[j] + part

    def first_rows(t):
        return xn[:, t * TILE:(t + 1) * TILE]

    def second_rows(t):
        return jnp.concatenate(
            [
                (x[i][:, t * TILE:(t + 1) * TILE].astype(F32) * roots[i]).astype(BF16)
                for i in range(per_seq, 2 * per_seq)
            ],
            axis=0,
        )

    eye = iota((16, 128), 0) == iota((16, 128), 1)

    def gates():
        bias_col = jnp.sum(jnp.where(eye, bias_row, 0.0), axis=1, keepdims=True)
        turned = acc_g[...].T
        logf = log_sigmoid(turned[16:32] + bias_col)
        lhs = jnp.concatenate(split3(logf), axis=0).astype(BF16)
        after = jnp.dot(lhs, tri[...], preferred_element_type=F32)
        rest = after[0:16] + after[16:32] + after[32:48]
        logw = rest + turned[0:16]
        top = jnp.max(logw, axis=1, keepdims=True)
        wrow[:, 0:span] = jnp.exp(logw - top)
        wrow[:, span:span + 128] = jnp.broadcast_to(rest[:, 0:1] + logf[:, 0:1], (16, 128))
        wrow[:, span + 128:span + 256] = jnp.broadcast_to(top, (16, 128))
        for h in range(2):
            mate_out[h:h + 1, :] = wrow[pl.ds(2 * mate + h, 1), :]

    def own_row_of(s, h):
        return wrow[pl.ds(2 * tp + h, 1), :] if s == 0 else mate_in[h:h + 1, :]

    def own_weight(s, h):
        return own_row_of(s, h)[:, 0:span]

    def normalizer(s, key):
        row = iota((16, span), 0)
        lhs = jnp.zeros((16, span), F32)
        for h in range(2):
            for i, part in enumerate(split3(own_weight(s, h))):
                lhs = jnp.where(row == 3 * h + i, part, lhs)
        out = jnp.dot(lhs.astype(BF16), key, preferred_element_type=F32)
        send_n[s][...] = jnp.concatenate(
            [out[0:1, 0:DH] + out[1:2, 0:DH] + out[2:3, 0:DH], out[3:4, DH:] + out[4:5, DH:] + out[5:6, DH:]], axis=0
        )

    def memory(s, value, key):
        mats = []
        for h in range(2):
            cols = slice(h * DH, (h + 1) * DH)
            turned = (value[:, cols].T.astype(F32) * own_weight(s, h)).astype(BF16)
            out = jnp.dot(turned, key[:, cols], preferred_element_type=F32)
            mats.append(out.reshape(16, 8, 128))
        low_half = iota((16, 8, 128), 1) < 4
        a, b = mats
        send_m[s][:, 0] = jnp.where(low_half, a, pltpu.roll(b, 4, 1)).astype(BF16)
        send_m[s][:, 1] = jnp.where(low_half, pltpu.roll(a, 4, 1), b).astype(BF16)

    def send_memory(s):
        for p in peers:
            pltpu.make_async_remote_copy(
                src_ref=send_m[s].at[p // 2, lax.rem(p, 2)], dst_ref=recv_m[s].at[sp],
                send_sem=sems.at[3 + s], recv_sem=msem.at[s],
                device_id=(p, tp), device_id_type=MESH,
            ).start()
            pltpu.make_async_remote_copy(
                src_ref=send_n[s], dst_ref=recv_n[s].at[sp],
                send_sem=sems.at[5 + s], recv_sem=nsem.at[s],
                device_id=(p, tp), device_id_type=MESH,
            ).start()
        recv_m[s][sp] = send_m[s][sp // 2, lax.rem(sp, 2)]
        recv_n[s][sp] = send_n[s][...]

    tiles = width // TILE
    roots, found = {}, {}

    def collected(i):
        roots[i] = jnp.concatenate([found[i, top] for top in range(0, ROWS, 16)], axis=0)

    land(x_loads[0])
    start(*x_loads[3:5])
    roots[0] = root(0, 0, ROWS)[0]
    land(gate_load, x_loads[1], *small)
    start(w_loads[1], x_loads[5])
    bias_row = jnp.concatenate([bias[...], jnp.zeros((1, 112), F32)], axis=1)
    gate([0], roots, squares_of(found, [1], 0, 8, 2))
    collected(1)
    land(x_loads[2])
    gate([1], roots, squares_of(found, [2], 0, 8, 2))
    collected(2)
    gate([2], roots)

    land(w_loads[0], *x_loads[3:5])
    start(load_q)
    sums_a, sums_b = [None, None], [None, None]
    project(first_rows, sums_a, range(tiles // 2), squares_of(found, [3, 4], 0, 8), {5: gates})
    land(w_loads[1], x_loads[5])
    handed = []

    def greet_and_hand():
        pl.semaphore_wait(barrier, SP - 1 + TP - 1)
        handed.append(pltpu.make_async_remote_copy(
            src_ref=mate_out, dst_ref=mate_in, send_sem=sems.at[9], recv_sem=mate_sem,
            device_id=(sp, mate), device_id_type=MESH,
        ))
        handed[0].start()

    def send_token():
        for p in tp_peers:
            pltpu.make_async_remote_copy(
                src_ref=fresh.at[tp], dst_ref=fresh.at[tp], send_sem=sems.at[8], recv_sem=new_sem,
                device_id=(sp, p), device_id_type=MESH,
            ).start()

    project(
        first_rows, sums_a, range(tiles // 2, tiles), squares_of(found, [5], tiles // 2, 8)
    )
    for i in range(per_seq, 2 * per_seq):
        collected(i)
    value_a, key_a = (total.astype(BF16) for total in sums_a)

    def first_memory():
        memory(0, value_a, key_a)
        normalizer(0, key_a)

    def scalars():
        lane = iota((1, 128), 1)
        line = jnp.zeros((1, 128), F32)
        for i in range(2):
            for q in range(4):
                own = own_row_of(q // 2, q % 2)[:, span + 128 * i:span + 128 * (i + 1)]
                line = jnp.where((lane >= 64 * i + 4 * q) & (lane < 64 * i + 4 * q + 4), own, line)
        send_s[...] = line
        recv_s[sp] = line

    def send_scalars():
        for p in peers:
            pltpu.make_async_remote_copy(
                src_ref=send_s, dst_ref=recv_s.at[sp], send_sem=sems.at[7], recv_sem=ssem,
                device_id=(p, tp), device_id_type=MESH,
            ).start()

    def arrived_scalars():
        handed[0].wait()
        scalars()

    between = {2: first_memory, 4: greet_and_hand, 5: lambda: send_memory(0), 9: send_token, 11: arrived_scalars, 13: send_scalars}
    project(second_rows, sums_b, range(tiles), None, between)
    value_b, key_b = (total.astype(BF16) for total in sums_b)
    normalizer(1, key_b)
    memory(1, value_b, key_b)
    send_memory(1)

    got = fresh.at[pl.ds(0, TP - 1)]
    pltpu.make_async_copy(got, got, sems.at[8]).wait()
    pltpu.make_async_copy(got, got, new_sem).wait()
    pieces = [fresh[k].astype(F32) for k in range(TP)]
    fresh_row = jnp.concatenate(pieces, axis=1)
    mean = jnp.sum(fresh_row * fresh_row, axis=1, keepdims=True) * (1.0 / width)
    token = (fresh_row * lax.rsqrt(mean + EPS)).astype(BF16)
    land(load_q)
    key = jnp.dot(token, w_vk[1], preferred_element_type=F32).astype(BF16).astype(F32)
    value = jnp.dot(token, w_vk[0], preferred_element_type=F32).astype(BF16).astype(F32)
    query = jnp.dot(token, wq[...], preferred_element_type=F32).astype(BF16).astype(F32)
    new_gate = lax.dot_general(token, wg[...], (((1,), (1,)), ((), ())), preferred_element_type=F32)

    def of_prompt(v, s):
        return jnp.where(order[s] == 0, v[0:1], v[1:2])

    def per_row(v, s):
        return jnp.concatenate(
            [jnp.broadcast_to(of_prompt(v, s)[:, h * DH:(h + 1) * DH], (4, DH)) for h in range(2)], axis=0
        )

    def picked(v, at):
        return jnp.sum(jnp.where(iota((8, v.shape[1]), 1) == at, v, 0.0), axis=1, keepdims=True)

    row8 = iota((8, 1), 0)
    own_row = 4 * sp + lax.rem(row8, 4)
    head = 2 * tp + row8 // 4
    bias_own = picked(jnp.broadcast_to(bias_row, (8, 128)), head)
    fresh_terms = []
    for s in range(2):
        q_rows, k_rows, v_rows = (per_row(v, s) for v in (query, key, value))
        agreement = jnp.sum(q_rows * k_rows, axis=1, keepdims=True)
        value_own = picked(v_rows, own_row)
        gate_rows = jnp.broadcast_to(of_prompt(new_gate, s), (8, 32))
        input_new = picked(gate_rows, head)
        forget_new = log_sigmoid(picked(gate_rows, 16 + head) + bias_own)
        fresh_terms.append((q_rows, agreement, value_own, input_new, forget_new))

    got = recv_s.at[pl.ds(0, SP - 1)]
    pltpu.make_async_copy(got, got, sems.at[7]).wait()
    pltpu.make_async_copy(got, got, ssem).wait()
    arrived = recv_s[:, 0, :]
    later = (iota((SP, SP), 1) > iota((SP, SP), 0)).astype(F32).astype(BF16)
    sums = jnp.dot(later, jnp.concatenate(split3(arrived), axis=1).astype(BF16), preferred_element_type=F32)
    lw = sums[:, 0:128] + sums[:, 128:256] + sums[:, 256:384] + pltpu.roll(arrived, 64, 1)
    top = jnp.max(lw, axis=0, keepdims=True)
    scale = jnp.exp(lw - top)
    stacked = jnp.concatenate([scale, jnp.broadcast_to(top, (8, 128)), jnp.zeros((88, 128), F32)], axis=0)
    turned = stacked.T

    factor = DH ** (-0.5)
    lane8 = iota((8, 128), 1)
    for s in range(2):
        q_rows, agreement, value_own, input_new, forget_new = fresh_terms[s]
        top_col = turned[8 * s:8 * s + 8, SP:SP + 1]
        share = turned[8 * s:8 * s + 8, 0:SP]
        top_next = jnp.maximum(forget_new + top_col, input_new)
        old_share = jnp.exp(forget_new + top_col - top_next)
        new_share = jnp.exp(input_new - top_next)
        shares = [jnp.broadcast_to(share[:, d:d + 1], (8, 128)) for d in range(SP)]
        scales = [jnp.broadcast_to(scale[:, 8 * s + 4 * h:8 * s + 4 * h + 1], (SP, 128)) for h in range(2)]
        got = recv_m[s].at[pl.ds(0, SP - 1)]
        pltpu.make_async_copy(got, got, sems.at[3 + s]).wait()
        pltpu.make_async_copy(got, got, msem.at[s]).wait()
        got = recv_n[s].at[pl.ds(0, SP - 1)]
        pltpu.make_async_copy(got, got, sems.at[5 + s]).wait()
        pltpu.make_async_copy(got, got, nsem.at[s]).wait()
        merged = [jnp.zeros((8, 128), F32) for _ in range(4)]
        for d in range(SP):
            merged[d % 4] = merged[d % 4] + shares[d] * recv_m[s][d].astype(F32)
        merged = (merged[0] + merged[1]) + (merged[2] + merged[3])
        matrix = merged.astype(BF16)
        n_rows = []
        for h in range(2):
            normal = jnp.sum(scales[h] * recv_n[s][:, h, :], axis=0, keepdims=True)
            n_rows.append(jnp.broadcast_to(normal, (4, 128)))
        n_rows = jnp.concatenate(n_rows, axis=0)
        numer = jnp.sum(matrix.astype(F32) * q_rows, axis=1, keepdims=True)
        numer = (old_share * numer + new_share * agreement * value_own) * factor
        denom = jnp.sum(n_rows * q_rows, axis=1, keepdims=True)
        denom = (old_share * denom + new_share * agreement) * factor
        read = numer / jnp.maximum(jnp.abs(denom), 1.0)
        own_normal = picked(n_rows, own_row)
        at = pl.ds(pl.multiple_of(8 * order[s], 8), 8)
        table[at, :] = jnp.where(lane8 == 0, own_normal, jnp.where(lane8 == 1, top_col, read))
        packed_out[at, :] = merged
    packed_out[16:24] = jnp.concatenate([table[...], jnp.zeros((112, 128), F32)], axis=0).T[0:8]


def unpack(packed, mat_out, nrm_out, top_out, read_out):
    for q in range(4):
        s, h = q // 2, q % 2
        lanes = slice(4 * q, 4 * q + 4)
        mat_out[s, h] = packed[lanes].astype(BF16)
        nrm_out[s, h:h + 1, :] = packed[16:17, lanes]
        top_out[s:s + 1, h:h + 1] = packed[17:18, 4 * q:4 * q + 1]
        read_out[s, h:h + 1, :] = packed[18:19, lanes].astype(BF16)


def shards(inputs, w_key, w_value, w_query, w_igate, w_fgate, forget_bias, new_rows):
    seqs, span, width = inputs.shape
    rows = seqs * span
    heads = w_key.shape[1] // DH
    out_shape = (
        jax.ShapeDtypeStruct((seqs, heads, DH // SP, DH), BF16),
        jax.ShapeDtypeStruct((seqs, heads, DH // SP), F32),
        jax.ShapeDtypeStruct((seqs, heads), F32),
        jax.ShapeDtypeStruct((seqs, heads, DH // SP), BF16),
    )
    hbm = pl.BlockSpec(memory_space=pl.ANY)
    vmem = pl.BlockSpec(memory_space=pltpu.VMEM)
    dma = pltpu.SemaphoreType.DMA
    packed = pl.pallas_call(
        kernel,
        out_shape=pltpu.VMEM((24, 128), F32),
        in_specs=[hbm] * 8,
        out_specs=vmem,
        scratch_shapes=[
            [pltpu.VMEM((ROWS, width), BF16) for _ in range(rows // ROWS)],
            pltpu.VMEM((span, width), BF16),
            pltpu.VMEM((2, width, heads * DH), BF16),
            pltpu.VMEM((width, heads * DH), BF16),
            pltpu.VMEM((32, width), BF16),
            pltpu.VMEM((1, 16), F32),
            pltpu.VMEM((TP, seqs, width // TP), BF16),
            pltpu.VMEM((span, 128), F32),
            pltpu.VMEM((span, span), BF16),
            pltpu.VMEM((16, span + 256), F32),
            pltpu.VMEM((2, span + 256), F32),
            pltpu.VMEM((2, span + 256), F32),
            pltpu.VMEM((16, 128), F32),
            [pltpu.VMEM((SP // 2, 2, MSG, 128), BF16) for _ in range(seqs)],
            [pltpu.VMEM((SP, MSG, 128), BF16) for _ in range(seqs)],
            [pltpu.VMEM((2, 128), F32) for _ in range(seqs)],
            [pltpu.VMEM((SP, 2, 128), F32) for _ in range(seqs)],
            pltpu.VMEM((1, 128), F32),
            pltpu.VMEM((SP, 1, 128), F32),
            dma((10,)),
            dma,
            dma,
            dma((seqs,)),
            dma((seqs,)),
            dma,
        ],
        compiler_params=pltpu.CompilerParams(
            collective_id=0, has_side_effects=True, vmem_limit_bytes=60 * 1024 * 1024
        ),
    )(
        inputs.reshape(rows, width), w_key, w_value, w_query,
        w_igate.T, w_fgate.T, forget_bias.reshape(1, -1), new_rows,
    )
    return pl.pallas_call(unpack, out_shape=out_shape, in_specs=[vmem], out_specs=[vmem] * 4)(
        pltpu.with_memory_space_constraint(packed, pltpu.VMEM)
    )


def solution(mesh):
    in_specs = (
        P(None, "sp", None),
        P(None, "tp"),
        P(None, "tp"),
        P(None, "tp"),
        P(),
        P(),
        P(),
        P(None, "tp"),
    )
    out_specs = (P(None, "tp", "sp", None), P(None, "tp", "sp"), P(None, "tp"), P(None, "tp", "sp"))
    return jax.shard_map(shards, mesh=mesh, in_specs=in_specs, out_specs=out_specs, check_vma=False)
```

```python
import functools

import jax
import jax.numpy as jnp
from jax import lax
from jax.experimental import pallas as pl
from jax.experimental.pallas import tpu as pltpu
from jax.sharding import PartitionSpec as P

DH = 128
EPS = 1e-06
MESH = pl.DeviceIdType.MESH
F32 = jnp.float32
BF16 = jnp.bfloat16
NZ, NY = 8, 4
SP, TP = NZ * NY, 8
ROWS = 128
TILE = 256
MSG = 8


def peer_offsets():
    offsets = [(dz, dy) for dz in range(NZ) for dy in range(NY) if dz or dy]
    return sorted(offsets, key=lambda o: -(min(o[0], NZ - o[0]) + min(o[1], NY - o[1])))


def iota(shape, dim):
    return lax.broadcasted_iota(jnp.int32, shape, dim)


def log_sigmoid(v):
    u = jnp.exp(-jnp.abs(v))
    series = u * (1.0 - u * (0.5 - u * (1.0 / 3.0 - u * (0.25 - u * (0.2 - u * (1.0 / 6.0))))))
    return jnp.minimum(v, 0.0) - jnp.where(u < 0.03, series, jnp.log(1.0 + u))


def split3(v):
    hi = v.astype(BF16).astype(F32)
    rest = v - hi
    mid = rest.astype(BF16).astype(F32)
    return hi, mid, rest - mid


def kernel(
    x_hbm, wk_hbm, wv_hbm, wq_hbm, wi_hbm, wf_hbm, bias_hbm, new_hbm,
    packed_out,
    x, xn, w_vk, wq, wg, bias, fresh, acc_g, tri, wrow, mate_out, mate_in, table,
    send_m, recv_m, send_n, recv_n, send_s, recv_s,
    sems, mate_sem, new_sem, msem, nsem, ssem,
):
    sp, tp = lax.axis_index("sp"), lax.axis_index("tp")
    z, y = sp // NY, lax.rem(sp, NY)
    span, width = xn.shape
    per_seq = span // ROWS
    peers = []
    for dz, dy in peer_offsets():
        peers.append(lax.rem(z + dz, NZ) * NY + lax.rem(y + dy, NY))
    core = lax.rem(tp, 2)
    order = core, 1 - core
    mate = tp + 1 - 2 * core
    tp_peers = [lax.rem(tp + k, TP) for k in range(1, TP)]

    def load(hbm, vmem, sem, parts):
        each = vmem.shape[0] // parts
        copies = []
        for i in range(parts):
            part = pl.ds(i * each, each)
            copies.append(pltpu.make_async_copy(hbm.at[part], vmem.at[part], sem))
        return copies, pltpu.make_async_copy(hbm, vmem, sem)

    def start(*loads):
        for copies, _ in loads:
            for copy in copies:
                copy.start()

    def land(*loads):
        for _, whole in loads:
            whole.wait()

    gate_load = (
        [
            pltpu.make_async_copy(wi_hbm, wg.at[pl.ds(0, 16)], sems.at[6]),
            pltpu.make_async_copy(wf_hbm, wg.at[pl.ds(16, 16)], sems.at[6]),
        ],
        pltpu.make_async_copy(wg, wg, sems.at[6]),
    )
    small = [load(bias_hbm, bias, sems.at[7], 1), load(new_hbm, fresh.at[tp], sems.at[8], 1)]
    x_loads = [
        load(
            x_hbm.at[pl.ds(pl.multiple_of(order[i // per_seq] * span + i % per_seq * ROWS, ROWS), ROWS)],
            x[i], sems.at[i], 8,
        )
        for i in range(2 * per_seq)
    ]
    half = width // 2
    w_loads = []
    for i in range(2):
        part, w_sem = pl.ds(i * half, half), sems.at[(9, 1)[i]]
        copies = []
        for j, hbm in enumerate((wv_hbm, wk_hbm)):
            copies += load(hbm.at[part], w_vk.at[j, part], w_sem, 4)[0]
        w_loads.append((copies, pltpu.make_async_copy(w_vk.at[:, part], w_vk.at[:, part], w_sem)))
    load_q = load(wq_hbm, wq, sems.at[2], 4)
    start(gate_load, x_loads[0], *small)

    barrier = pltpu.get_barrier_semaphore()
    for p in peers:
        pl.semaphore_signal(barrier, inc=1, device_id=(p, tp), device_id_type=MESH)
    for p in tp_peers:
        pl.semaphore_signal(barrier, inc=1, device_id=(sp, p), device_id_type=MESH)
    start(*x_loads[1:3])
    tri[...] = (iota((span, span), 0) > iota((span, span), 1)).astype(F32).astype(BF16)
    start(w_loads[0])

    def root(i, top, count):
        total = None
        for c in range(0, width, 128):
            piece = x[i][top:top + count, c:c + 128].astype(F32)
            total = piece * piece if total is None else total + piece * piece
        mean = jnp.sum(total, axis=1, keepdims=True) * (1.0 / width)
        return lax.rsqrt(mean + EPS), total

    def gate(blocks, roots, squares=None, between=None):
        totals = {}
        for t in range(width // TILE):
            c = t * TILE
            if between and t in between:
                between[t]()
            for i in blocks:
                at = i * ROWS
                normed = (x[i][:, c:c + TILE].astype(F32) * roots[i]).astype(BF16)
                xn[at:at + ROWS, c:c + TILE] = normed
                zero = squares(t) if squares else None
                if zero is not None:
                    normed = jnp.concatenate([normed[0:16] + zero, normed[16:]], axis=0)
                for half_of in range(2):
                    top = half_of * ROWS // 2
                    part = lax.dot_general(
                        normed[top:top + ROWS // 2], wg[:, c:c + TILE],
                        (((1,), (1,)), ((), ())), preferred_element_type=F32,
                    )
                    key = i, half_of
                    totals[key] = part if key not in totals else totals[key] + part
        for (i, half_of), total in totals.items():
            at = i * ROWS + half_of * ROWS // 2
            acc_g[at:at + ROWS // 2, 0:32] = total

    def squares_of(found, blocks, first, count, stride=1):
        groups = [(i, top) for i in blocks for top in range(0, ROWS, 16)]
        share = len(groups) // count

        def squares(t):
            at, odd = divmod(t - first, stride)
            if odd or not 0 <= at < count:
                return None
            zero = None
            for i, top in groups[at * share:(at + 1) * share]:
                found[i, top], total = root(i, top, 16)
                low = jnp.minimum(total, 0.0)
                zero = low if zero is None else zero + low
            return jnp.concatenate([zero, zero], axis=1).astype(BF16)

        return squares

    def project(normed, sums, tiles, squares=None, between=None):
        for t in tiles:
            if between and t in between:
                between[t]()
            rows_n = normed(t)
            zero = squares(t) if squares else None
            if zero is not None:
                rows_n = jnp.concatenate([rows_n[0:16] + zero, rows_n[16:]], axis=0)
            for j in range(2):
                part = jnp.dot(rows_n, w_vk[j, t * TILE:(t + 1) * TILE, :], preferred_element_type=F32)
                sums[j] = part if sums[j] is None else sums[j] + part

    def first_rows(t):
        return xn[:, t * TILE:(t + 1) * TILE]

    def second_rows(t):
        return jnp.concatenate(
            [
                (x[i][:, t * TILE:(t + 1) * TILE].astype(F32) * roots[i]).astype(BF16)
                for i in range(per_seq, 2 * per_seq)
            ],
            axis=0,
        )

    eye = iota((16, 128), 0) == iota((16, 128), 1)

    def gates():
        bias_col = jnp.sum(jnp.where(eye, bias_row, 0.0), axis=1, keepdims=True)
        turned = acc_g[...].T
        logf = log_sigmoid(turned[16:32] + bias_col)
        lhs = jnp.concatenate(split3(logf), axis=0).astype(BF16)
        after = jnp.dot(lhs, tri[...], preferred_element_type=F32)
        rest = after[0:16] + after[16:32] + after[32:48]
        logw = rest + turned[0:16]
        top = jnp.max(logw, axis=1, keepdims=True)
        wrow[:, 0:span] = jnp.exp(logw - top)
        wrow[:, span:span + 128] = jnp.broadcast_to(rest[:, 0:1] + logf[:, 0:1], (16, 128))
        wrow[:, span + 128:span + 256] = jnp.broadcast_to(top, (16, 128))
        for h in range(2):
            mate_out[h:h + 1, :] = wrow[pl.ds(2 * mate + h, 1), :]

    def own_row_of(s, h):
        return wrow[pl.ds(2 * tp + h, 1), :] if s == 0 else mate_in[h:h + 1, :]

    def own_weight(s, h):
        return own_row_of(s, h)[:, 0:span]

    def normalizer(s, key):
        row = iota((16, span), 0)
        lhs = jnp.zeros((16, span), F32)
        for h in range(2):
            for i, part in enumerate(split3(own_weight(s, h))):
                lhs = jnp.where(row == 3 * h + i, part, lhs)
        out = jnp.dot(lhs.astype(BF16), key, preferred_element_type=F32)
        send_n[s][...] = jnp.concatenate(
            [out[0:1, 0:DH] + out[1:2, 0:DH] + out[2:3, 0:DH], out[3:4, DH:] + out[4:5, DH:] + out[5:6, DH:]], axis=0
        )

    def memory(s, value, key):
        mats = []
        for h in range(2):
            cols = slice(h * DH, (h + 1) * DH)
            turned = (value[:, cols].T.astype(F32) * own_weight(s, h)).astype(BF16)
            out = jnp.dot(turned, key[:, cols], preferred_element_type=F32)
            mats.append(out.reshape(16, 8, 128))
        low_half = iota((16, 8, 128), 1) < 4
        a, b = mats
        send_m[s][:, 0] = jnp.where(low_half, a, pltpu.roll(b, 4, 1)).astype(BF16)
        send_m[s][:, 1] = jnp.where(low_half, pltpu.roll(a, 4, 1), b).astype(BF16)

    def send_memory(s):
        for p in peers:
            pltpu.make_async_remote_copy(
                src_ref=send_m[s].at[p // 2, lax.rem(p, 2)], dst_ref=recv_m[s].at[sp],
                send_sem=sems.at[3 + s], recv_sem=msem.at[s],
                device_id=(p, tp), device_id_type=MESH,
            ).start()
            pltpu.make_async_remote_copy(
                src_ref=send_n[s], dst_ref=recv_n[s].at[sp],
                send_sem=sems.at[5 + s], recv_sem=nsem.at[s],
                device_id=(p, tp), device_id_type=MESH,
            ).start()
        recv_m[s][sp] = send_m[s][sp // 2, lax.rem(sp, 2)]
        recv_n[s][sp] = send_n[s][...]

    tiles = width // TILE
    roots, found = {}, {}

    def collected(i):
        roots[i] = jnp.concatenate([found[i, top] for top in range(0, ROWS, 16)], axis=0)

    land(x_loads[0])
    start(x_loads[3])
    roots[0] = root(0, 0, ROWS)[0]
    land(gate_load, x_loads[1], *small)
    start(w_loads[1], *x_loads[4:])
    bias_row = jnp.concatenate([bias[...], jnp.zeros((1, 112), F32)], axis=1)
    gate([0], roots, squares_of(found, [1], 0, 8, 2))
    collected(1)
    land(x_loads[2])
    gate([1], roots, squares_of(found, [2], 0, 8, 2))
    collected(2)
    gate([2], roots)

    land(w_loads[0], x_loads[3])
    start(load_q)
    sums_a, sums_b = [None, None], [None, None]
    project(first_rows, sums_a, range(tiles // 2), squares_of(found, [3], 0, 8), {5: gates})
    land(w_loads[1], *x_loads[4:])
    handed = []

    def greet_and_hand():
        pl.semaphore_wait(barrier, SP - 1 + TP - 1)
        handed.append(pltpu.make_async_remote_copy(
            src_ref=mate_out, dst_ref=mate_in, send_sem=sems.at[9], recv_sem=mate_sem,
            device_id=(sp, mate), device_id_type=MESH,
        ))
        handed[0].start()

    def send_token():
        for p in tp_peers:
            pltpu.make_async_remote_copy(
                src_ref=fresh.at[tp], dst_ref=fresh.at[tp], send_sem=sems.at[8], recv_sem=new_sem,
                device_id=(sp, p), device_id_type=MESH,
            ).start()

    project(
        first_rows, sums_a, range(tiles // 2, tiles), squares_of(found, [4, 5], tiles // 2, 8)
    )
    for i in range(per_seq, 2 * per_seq):
        collected(i)
    value_a, key_a = (total.astype(BF16) for total in sums_a)

    def first_memory():
        memory(0, value_a, key_a)
        normalizer(0, key_a)

    def scalars():
        lane = iota((1, 128), 1)
        line = jnp.zeros((1, 128), F32)
        for i in range(2):
            for q in range(4):
                own = own_row_of(q // 2, q % 2)[:, span + 128 * i:span + 128 * (i + 1)]
                line = jnp.where((lane >= 64 * i + 4 * q) & (lane < 64 * i + 4 * q + 4), own, line)
        send_s[...] = line
        recv_s[sp] = line

    def send_scalars():
        for p in peers:
            pltpu.make_async_remote_copy(
                src_ref=send_s, dst_ref=recv_s.at[sp], send_sem=sems.at[7], recv_sem=ssem,
                device_id=(p, tp), device_id_type=MESH,
            ).start()

    def arrived_scalars():
        handed[0].wait()
        scalars()

    greet_and_hand()
    between = {1: first_memory, 3: lambda: send_memory(0), 8: arrived_scalars, 9: send_scalars, 12: send_token}
    project(second_rows, sums_b, range(tiles), None, between)
    value_b, key_b = (total.astype(BF16) for total in sums_b)
    normalizer(1, key_b)
    memory(1, value_b, key_b)
    send_memory(1)

    got = fresh.at[pl.ds(0, TP - 1)]
    pltpu.make_async_copy(got, got, sems.at[8]).wait()
    pltpu.make_async_copy(got, got, new_sem).wait()
    pieces = [fresh[k].astype(F32) for k in range(TP)]
    fresh_row = jnp.concatenate(pieces, axis=1)
    mean = jnp.sum(fresh_row * fresh_row, axis=1, keepdims=True) * (1.0 / width)
    token = (fresh_row * lax.rsqrt(mean + EPS)).astype(BF16)
    land(load_q)
    key = jnp.dot(token, w_vk[1], preferred_element_type=F32).astype(BF16).astype(F32)
    value = jnp.dot(token, w_vk[0], preferred_element_type=F32).astype(BF16).astype(F32)
    query = jnp.dot(token, wq[...], preferred_element_type=F32).astype(BF16).astype(F32)
    new_gate = lax.dot_general(token, wg[...], (((1,), (1,)), ((), ())), preferred_element_type=F32)

    def of_prompt(v, s):
        return jnp.where(order[s] == 0, v[0:1], v[1:2])

    def per_row(v, s):
        return jnp.concatenate(
            [jnp.broadcast_to(of_prompt(v, s)[:, h * DH:(h + 1) * DH], (4, DH)) for h in range(2)], axis=0
        )

    def picked(v, at):
        return jnp.sum(jnp.where(iota((8, v.shape[1]), 1) == at, v, 0.0), axis=1, keepdims=True)

    row8 = iota((8, 1), 0)
    own_row = 4 * sp + lax.rem(row8, 4)
    head = 2 * tp + row8 // 4
    bias_own = picked(jnp.broadcast_to(bias_row, (8, 128)), head)
    fresh_terms = []
    for s in range(2):
        q_rows, k_rows, v_rows = (per_row(v, s) for v in (query, key, value))
        agreement = jnp.sum(q_rows * k_rows, axis=1, keepdims=True)
        value_own = picked(v_rows, own_row)
        gate_rows = jnp.broadcast_to(of_prompt(new_gate, s), (8, 32))
        input_new = picked(gate_rows, head)
        forget_new = log_sigmoid(picked(gate_rows, 16 + head) + bias_own)
        fresh_terms.append((q_rows, agreement, value_own, input_new, forget_new))

    got = recv_s.at[pl.ds(0, SP - 1)]
    pltpu.make_async_copy(got, got, sems.at[7]).wait()
    pltpu.make_async_copy(got, got, ssem).wait()
    arrived = recv_s[:, 0, :]
    later = (iota((SP, SP), 1) > iota((SP, SP), 0)).astype(F32).astype(BF16)
    sums = jnp.dot(later, jnp.concatenate(split3(arrived), axis=1).astype(BF16), preferred_element_type=F32)
    lw = sums[:, 0:128] + sums[:, 128:256] + sums[:, 256:384] + pltpu.roll(arrived, 64, 1)
    top = jnp.max(lw, axis=0, keepdims=True)
    scale = jnp.exp(lw - top)
    stacked = jnp.concatenate([scale, jnp.broadcast_to(top, (8, 128))], axis=0)
    turned = stacked.T

    factor = DH ** (-0.5)
    lane8 = iota((8, 128), 1)
    for s in range(2):
        q_rows, agreement, value_own, input_new, forget_new = fresh_terms[s]
        top_col = turned[8 * s:8 * s + 8, SP:SP + 1]
        share = turned[8 * s:8 * s + 8, 0:SP]
        top_next = jnp.maximum(forget_new + top_col, input_new)
        old_share = jnp.exp(forget_new + top_col - top_next)
        new_share = jnp.exp(input_new - top_next)
        shares = [jnp.broadcast_to(share[:, d:d + 1], (8, 128)) for d in range(SP)]
        scales = [jnp.broadcast_to(scale[:, 8 * s + 4 * h:8 * s + 4 * h + 1], (SP, 128)) for h in range(2)]
        got = recv_m[s].at[pl.ds(0, SP - 1)]
        pltpu.make_async_copy(got, got, sems.at[3 + s]).wait()
        pltpu.make_async_copy(got, got, msem.at[s]).wait()
        got = recv_n[s].at[pl.ds(0, SP - 1)]
        pltpu.make_async_copy(got, got, sems.at[5 + s]).wait()
        pltpu.make_async_copy(got, got, nsem.at[s]).wait()
        merged = [jnp.zeros((8, 128), F32) for _ in range(4)]
        for d in range(SP):
            merged[d % 4] = merged[d % 4] + shares[d] * recv_m[s][d].astype(F32)
        merged = (merged[0] + merged[1]) + (merged[2] + merged[3])
        matrix = merged.astype(BF16)
        n_rows = []
        for h in range(2):
            normal = jnp.sum(scales[h] * recv_n[s][:, h, :], axis=0, keepdims=True)
            n_rows.append(jnp.broadcast_to(normal, (4, 128)))
        n_rows = jnp.concatenate(n_rows, axis=0)
        numer = jnp.sum(matrix.astype(F32) * q_rows, axis=1, keepdims=True)
        numer = (old_share * numer + new_share * agreement * value_own) * factor
        denom = jnp.sum(n_rows * q_rows, axis=1, keepdims=True)
        denom = (old_share * denom + new_share * agreement) * factor
        read = numer / jnp.maximum(jnp.abs(denom), 1.0)
        own_normal = picked(n_rows, own_row)
        at = pl.ds(pl.multiple_of(8 * order[s], 8), 8)
        table[at, :] = jnp.where(lane8 == 0, own_normal, jnp.where(lane8 == 1, top_col, read))
        packed_out[at, :] = merged
    packed_out[16:24] = jnp.concatenate([table[...], jnp.zeros((112, 128), F32)], axis=0).T[0:8]


def unpack(packed, mat_out, nrm_out, top_out, read_out):
    for q in range(4):
        s, h = q // 2, q % 2
        lanes = slice(4 * q, 4 * q + 4)
        mat_out[s, h] = packed[lanes].astype(BF16)
        nrm_out[s, h:h + 1, :] = packed[16:17, lanes]
        top_out[s:s + 1, h:h + 1] = packed[17:18, 4 * q:4 * q + 1]
        read_out[s, h:h + 1, :] = packed[18:19, lanes].astype(BF16)


def shards(inputs, w_key, w_value, w_query, w_igate, w_fgate, forget_bias, new_rows):
    seqs, span, width = inputs.shape
    rows = seqs * span
    heads = w_key.shape[1] // DH
    out_shape = (
        jax.ShapeDtypeStruct((seqs, heads, DH // SP, DH), BF16),
        jax.ShapeDtypeStruct((seqs, heads, DH // SP), F32),
        jax.ShapeDtypeStruct((seqs, heads), F32),
        jax.ShapeDtypeStruct((seqs, heads, DH // SP), BF16),
    )
    hbm = pl.BlockSpec(memory_space=pl.ANY)
    vmem = pl.BlockSpec(memory_space=pltpu.VMEM)
    dma = pltpu.SemaphoreType.DMA
    packed = pl.pallas_call(
        kernel,
        out_shape=pltpu.VMEM((24, 128), F32),
        in_specs=[hbm] * 8,
        out_specs=vmem,
        scratch_shapes=[
            [pltpu.VMEM((ROWS, width), BF16) for _ in range(rows // ROWS)],
            pltpu.VMEM((span, width), BF16),
            pltpu.VMEM((2, width, heads * DH), BF16),
            pltpu.VMEM((width, heads * DH), BF16),
            pltpu.VMEM((32, width), BF16),
            pltpu.VMEM((1, 16), F32),
            pltpu.VMEM((TP, seqs, width // TP), BF16),
            pltpu.VMEM((span, 128), F32),
            pltpu.VMEM((span, span), BF16),
            pltpu.VMEM((16, span + 256), F32),
            pltpu.VMEM((2, span + 256), F32),
            pltpu.VMEM((2, span + 256), F32),
            pltpu.VMEM((16, 128), F32),
            [pltpu.VMEM((SP // 2, 2, MSG, 128), BF16) for _ in range(seqs)],
            [pltpu.VMEM((SP, MSG, 128), BF16) for _ in range(seqs)],
            [pltpu.VMEM((2, 128), F32) for _ in range(seqs)],
            [pltpu.VMEM((SP, 2, 128), F32) for _ in range(seqs)],
            pltpu.VMEM((1, 128), F32),
            pltpu.VMEM((SP, 1, 128), F32),
            dma((10,)),
            dma,
            dma,
            dma((seqs,)),
            dma((seqs,)),
            dma,
        ],
        compiler_params=pltpu.CompilerParams(
            collective_id=0, has_side_effects=True, vmem_limit_bytes=60 * 1024 * 1024
        ),
    )(
        inputs.reshape(rows, width), w_key, w_value, w_query,
        w_igate.T, w_fgate.T, forget_bias.reshape(1, -1), new_rows,
    )
    return pl.pallas_call(unpack, out_shape=out_shape, in_specs=[vmem], out_specs=[vmem] * 4)(
        pltpu.with_memory_space_constraint(packed, pltpu.VMEM)
    )


def solution(mesh):
    in_specs = (
        P(None, "sp", None),
        P(None, "tp"),
        P(None, "tp"),
        P(None, "tp"),
        P(),
        P(),
        P(),
        P(None, "tp"),
    )
    out_specs = (P(None, "tp", "sp", None), P(None, "tp", "sp"), P(None, "tp"), P(None, "tp", "sp"))
    return jax.shard_map(shards, mesh=mesh, in_specs=in_specs, out_specs=out_specs, check_vma=False)
```

```python
import functools

import jax
import jax.numpy as jnp
from jax import lax
from jax.experimental import pallas as pl
from jax.experimental.pallas import tpu as pltpu
from jax.sharding import PartitionSpec as P

DH = 128
EPS = 1e-06
MESH = pl.DeviceIdType.MESH
F32 = jnp.float32
BF16 = jnp.bfloat16
NZ, NY = 8, 4
SP, TP = NZ * NY, 8
ROWS = 128
TILE = 256
MSG = 8


def peer_offsets():
    offsets = [(dz, dy) for dz in range(NZ) for dy in range(NY) if dz or dy]
    return sorted(offsets, key=lambda o: -(min(o[0], NZ - o[0]) + min(o[1], NY - o[1])))


def iota(shape, dim):
    return lax.broadcasted_iota(jnp.int32, shape, dim)


def log_sigmoid(v):
    u = jnp.exp(-jnp.abs(v))
    series = u * (1.0 - u * (0.5 - u * (1.0 / 3.0 - u * (0.25 - u * (0.2 - u * (1.0 / 6.0))))))
    return jnp.minimum(v, 0.0) - jnp.where(u < 0.03, series, jnp.log(1.0 + u))


def split3(v):
    hi = v.astype(BF16).astype(F32)
    rest = v - hi
    mid = rest.astype(BF16).astype(F32)
    return hi, mid, rest - mid


def kernel(
    x_hbm, wk_hbm, wv_hbm, wq_hbm, wi_hbm, wf_hbm, bias_hbm, new_hbm,
    packed_out,
    x, xn, w_vk, wq, wg, bias, fresh, acc_g, tri, wrow, mate_out, mate_in, table,
    send_m, recv_m, send_n, recv_n, send_s, recv_s,
    sems, mate_sem, new_sem, msem, nsem, ssem,
):
    sp, tp = lax.axis_index("sp"), lax.axis_index("tp")
    z, y = sp // NY, lax.rem(sp, NY)
    span, width = xn.shape
    per_seq = span // ROWS
    peers = []
    for dz, dy in peer_offsets():
        peers.append(lax.rem(z + dz, NZ) * NY + lax.rem(y + dy, NY))
    core = lax.rem(tp, 2)
    order = core, 1 - core
    mate = tp + 1 - 2 * core
    tp_peers = [lax.rem(tp + k, TP) for k in range(1, TP)]

    def load(hbm, vmem, sem, parts):
        each = vmem.shape[0] // parts
        copies = []
        for i in range(parts):
            part = pl.ds(i * each, each)
            copies.append(pltpu.make_async_copy(hbm.at[part], vmem.at[part], sem))
        return copies, pltpu.make_async_copy(hbm, vmem, sem)

    def start(*loads):
        for copies, _ in loads:
            for copy in copies:
                copy.start()

    def land(*loads):
        for _, whole in loads:
            whole.wait()

    gate_load = (
        [
            pltpu.make_async_copy(wi_hbm, wg.at[pl.ds(0, 16)], sems.at[6]),
            pltpu.make_async_copy(wf_hbm, wg.at[pl.ds(16, 16)], sems.at[6]),
        ],
        pltpu.make_async_copy(wg, wg, sems.at[6]),
    )
    small = [load(bias_hbm, bias, sems.at[7], 1), load(new_hbm, fresh.at[tp], sems.at[8], 1)]
    x_loads = [
        load(
            x_hbm.at[pl.ds(pl.multiple_of(order[i // per_seq] * span + i % per_seq * ROWS, ROWS), ROWS)],
            x[i], sems.at[i], 8,
        )
        for i in range(2 * per_seq)
    ]
    half = width // 2
    w_loads = []
    for i in range(2):
        part, w_sem = pl.ds(i * half, half), sems.at[(9, 1)[i]]
        copies = []
        for j, hbm in enumerate((wv_hbm, wk_hbm)):
            copies += load(hbm.at[part], w_vk.at[j, part], w_sem, 4)[0]
        w_loads.append((copies, pltpu.make_async_copy(w_vk.at[:, part], w_vk.at[:, part], w_sem)))
    load_q = load(wq_hbm, wq, sems.at[2], 4)
    start(gate_load, x_loads[0], *small)

    barrier = pltpu.get_barrier_semaphore()
    for p in peers:
        pl.semaphore_signal(barrier, inc=1, device_id=(p, tp), device_id_type=MESH)
    for p in tp_peers:
        pl.semaphore_signal(barrier, inc=1, device_id=(sp, p), device_id_type=MESH)
    start(*x_loads[1:3])
    tri[...] = (iota((span, span), 0) > iota((span, span), 1)).astype(F32).astype(BF16)
    start(w_loads[0])

    def root(i, top, count):
        total = None
        for c in range(0, width, 128):
            piece = x[i][top:top + count, c:c + 128].astype(F32)
            total = piece * piece if total is None else total + piece * piece
        mean = jnp.sum(total, axis=1, keepdims=True) * (1.0 / width)
        return lax.rsqrt(mean + EPS), total

    def gate(blocks, roots, squares=None, between=None):
        totals = {}
        for t in range(width // TILE):
            c = t * TILE
            if between and t in between:
                between[t]()
            for i in blocks:
                at = i * ROWS
                normed = (x[i][:, c:c + TILE].astype(F32) * roots[i]).astype(BF16)
                xn[at:at + ROWS, c:c + TILE] = normed
                zero = squares(t) if squares else None
                if zero is not None:
                    normed = jnp.concatenate([normed[0:16] + zero, normed[16:]], axis=0)
                for half_of in range(2):
                    top = half_of * ROWS // 2
                    part = lax.dot_general(
                        normed[top:top + ROWS // 2], wg[:, c:c + TILE],
                        (((1,), (1,)), ((), ())), preferred_element_type=F32,
                    )
                    key = i, half_of
                    totals[key] = part if key not in totals else totals[key] + part
        for (i, half_of), total in totals.items():
            at = i * ROWS + half_of * ROWS // 2
            acc_g[at:at + ROWS // 2, 0:32] = total

    def squares_of(found, blocks, first, count, stride=1):
        groups = [(i, top) for i in blocks for top in range(0, ROWS, 16)]
        share = len(groups) // count

        def squares(t):
            at, odd = divmod(t - first, stride)
            if odd or not 0 <= at < count:
                return None
            zero = None
            for i, top in groups[at * share:(at + 1) * share]:
                found[i, top], total = root(i, top, 16)
                low = jnp.minimum(total, 0.0)
                zero = low if zero is None else zero + low
            return jnp.concatenate([zero, zero], axis=1).astype(BF16)

        return squares

    def project(normed, sums, tiles, squares=None, between=None):
        for t in tiles:
            if between and t in between:
                between[t]()
            rows_n = normed(t)
            zero = squares(t) if squares else None
            if zero is not None:
                rows_n = jnp.concatenate([rows_n[0:16] + zero, rows_n[16:]], axis=0)
            for j in range(2):
                part = jnp.dot(rows_n, w_vk[j, t * TILE:(t + 1) * TILE, :], preferred_element_type=F32)
                sums[j] = part if sums[j] is None else sums[j] + part

    def first_rows(t):
        return xn[:, t * TILE:(t + 1) * TILE]

    def second_rows(t):
        return jnp.concatenate(
            [
                (x[i][:, t * TILE:(t + 1) * TILE].astype(F32) * roots[i]).astype(BF16)
                for i in range(per_seq, 2 * per_seq)
            ],
            axis=0,
        )

    eye = iota((16, 128), 0) == iota((16, 128), 1)

    def gates():
        bias_col = jnp.sum(jnp.where(eye, bias_row, 0.0), axis=1, keepdims=True)
        turned = acc_g[...].T
        logf = log_sigmoid(turned[16:32] + bias_col)
        lhs = jnp.concatenate(split3(logf), axis=0).astype(BF16)
        after = jnp.dot(lhs, tri[...], preferred_element_type=F32)
        rest = after[0:16] + after[16:32] + after[32:48]
        logw = rest + turned[0:16]
        top = jnp.max(logw, axis=1, keepdims=True)
        wrow[:, 0:span] = jnp.exp(logw - top)
        wrow[:, span:span + 128] = jnp.broadcast_to(rest[:, 0:1] + logf[:, 0:1], (16, 128))
        wrow[:, span + 128:span + 256] = jnp.broadcast_to(top, (16, 128))
        for h in range(2):
            mate_out[h:h + 1, :] = wrow[pl.ds(2 * mate + h, 1), :]

    def own_row_of(s, h):
        return wrow[pl.ds(2 * tp + h, 1), :] if s == 0 else mate_in[h:h + 1, :]

    def own_weight(s, h):
        return own_row_of(s, h)[:, 0:span]

    def normalizer(s, key):
        row = iota((16, span), 0)
        lhs = jnp.zeros((16, span), F32)
        for h in range(2):
            for i, part in enumerate(split3(own_weight(s, h))):
                lhs = jnp.where(row == 3 * h + i, part, lhs)
        out = jnp.dot(lhs.astype(BF16), key, preferred_element_type=F32)
        send_n[s][...] = jnp.concatenate(
            [out[0:1, 0:DH] + out[1:2, 0:DH] + out[2:3, 0:DH], out[3:4, DH:] + out[4:5, DH:] + out[5:6, DH:]], axis=0
        )

    def memory(s, value, key):
        mats = []
        for h in range(2):
            cols = slice(h * DH, (h + 1) * DH)
            turned = (value[:, cols].T.astype(F32) * own_weight(s, h)).astype(BF16)
            out = jnp.dot(turned, key[:, cols], preferred_element_type=F32)
            mats.append(out.reshape(16, 8, 128))
        low_half = iota((16, 8, 128), 1) < 4
        a, b = mats
        send_m[s][:, 0] = jnp.where(low_half, a, pltpu.roll(b, 4, 1)).astype(BF16)
        send_m[s][:, 1] = jnp.where(low_half, pltpu.roll(a, 4, 1), b).astype(BF16)

    def send_memory(s):
        for p in peers:
            pltpu.make_async_remote_copy(
                src_ref=send_m[s].at[p // 2, lax.rem(p, 2)], dst_ref=recv_m[s].at[sp],
                send_sem=sems.at[3 + s], recv_sem=msem.at[s],
                device_id=(p, tp), device_id_type=MESH,
            ).start()
            pltpu.make_async_remote_copy(
                src_ref=send_n[s], dst_ref=recv_n[s].at[sp],
                send_sem=sems.at[5 + s], recv_sem=nsem.at[s],
                device_id=(p, tp), device_id_type=MESH,
            ).start()
        recv_m[s][sp] = send_m[s][sp // 2, lax.rem(sp, 2)]
        recv_n[s][sp] = send_n[s][...]

    tiles = width // TILE
    roots, found = {}, {}

    def collected(i):
        roots[i] = jnp.concatenate([found[i, top] for top in range(0, ROWS, 16)], axis=0)

    land(x_loads[0])
    start(x_loads[3])
    roots[0] = root(0, 0, ROWS)[0]
    land(gate_load, x_loads[1], *small)
    start(w_loads[1], *x_loads[4:])
    bias_row = jnp.concatenate([bias[...], jnp.zeros((1, 112), F32)], axis=1)
    gate([0], roots, squares_of(found, [1], 0, 8, 2))
    collected(1)
    land(x_loads[2])
    gate([1], roots, squares_of(found, [2], 0, 8, 2))
    collected(2)
    gate([2], roots)

    land(w_loads[0], x_loads[3])
    start(load_q)
    sums_a, sums_b = [None, None], [None, None]
    project(first_rows, sums_a, range(tiles // 2), squares_of(found, [3], 0, 8), {5: gates})
    land(w_loads[1], *x_loads[4:])
    handed = []

    def greet_and_hand():
        pl.semaphore_wait(barrier, SP - 1 + TP - 1)
        handed.append(pltpu.make_async_remote_copy(
            src_ref=mate_out, dst_ref=mate_in, send_sem=sems.at[9], recv_sem=mate_sem,
            device_id=(sp, mate), device_id_type=MESH,
        ))
        handed[0].start()

    def send_token():
        for p in tp_peers:
            pltpu.make_async_remote_copy(
                src_ref=fresh.at[tp], dst_ref=fresh.at[tp], send_sem=sems.at[8], recv_sem=new_sem,
                device_id=(sp, p), device_id_type=MESH,
            ).start()

    project(
        first_rows, sums_a, range(tiles // 2, tiles), squares_of(found, [4, 5], tiles // 2, 8)
    )
    for i in range(per_seq, 2 * per_seq):
        collected(i)
    value_a, key_a = (total.astype(BF16) for total in sums_a)

    def first_memory():
        memory(0, value_a, key_a)
        normalizer(0, key_a)

    def scalars():
        lane = iota((1, 128), 1)
        line = jnp.zeros((1, 128), F32)
        for i in range(2):
            for q in range(4):
                own = own_row_of(q // 2, q % 2)[:, span + 128 * i:span + 128 * (i + 1)]
                line = jnp.where((lane >= 64 * i + 4 * q) & (lane < 64 * i + 4 * q + 4), own, line)
        send_s[...] = line
        recv_s[sp] = line

    def send_scalars():
        for p in peers:
            pltpu.make_async_remote_copy(
                src_ref=send_s, dst_ref=recv_s.at[sp], send_sem=sems.at[7], recv_sem=ssem,
                device_id=(p, tp), device_id_type=MESH,
            ).start()

    def arrived_scalars():
        handed[0].wait()
        scalars()

    greet_and_hand()
    between = {1: first_memory, 3: lambda: send_memory(0), 8: arrived_scalars, 9: send_scalars, 12: send_token}
    project(second_rows, sums_b, range(tiles), None, between)
    value_b, key_b = (total.astype(BF16) for total in sums_b)
    normalizer(1, key_b)
    memory(1, value_b, key_b)
    send_memory(1)

    got = fresh.at[pl.ds(0, TP - 1)]
    pltpu.make_async_copy(got, got, sems.at[8]).wait()
    pltpu.make_async_copy(got, got, new_sem).wait()
    pieces = [fresh[k].astype(F32) for k in range(TP)]
    fresh_row = jnp.concatenate(pieces, axis=1)
    mean = jnp.sum(fresh_row * fresh_row, axis=1, keepdims=True) * (1.0 / width)
    token = (fresh_row * lax.rsqrt(mean + EPS)).astype(BF16)
    land(load_q)
    key = jnp.dot(token, w_vk[1], preferred_element_type=F32).astype(BF16).astype(F32)
    value = jnp.dot(token, w_vk[0], preferred_element_type=F32).astype(BF16).astype(F32)
    query = jnp.dot(token, wq[...], preferred_element_type=F32).astype(BF16).astype(F32)
    new_gate = lax.dot_general(token, wg[...], (((1,), (1,)), ((), ())), preferred_element_type=F32)

    def of_prompt(v, s):
        return jnp.where(order[s] == 0, v[0:1], v[1:2])

    def per_row(v, s):
        return jnp.concatenate(
            [jnp.broadcast_to(of_prompt(v, s)[:, h * DH:(h + 1) * DH], (4, DH)) for h in range(2)], axis=0
        )

    def picked(v, at):
        return jnp.sum(jnp.where(iota((8, v.shape[1]), 1) == at, v, 0.0), axis=1, keepdims=True)

    row8 = iota((8, 1), 0)
    own_row = 4 * sp + lax.rem(row8, 4)
    head = 2 * tp + row8 // 4
    bias_own = picked(jnp.broadcast_to(bias_row, (8, 128)), head)
    fresh_terms = []
    for s in range(2):
        q_rows, k_rows, v_rows = (per_row(v, s) for v in (query, key, value))
        agreement = jnp.sum(q_rows * k_rows, axis=1, keepdims=True)
        value_own = picked(v_rows, own_row)
        gate_rows = jnp.broadcast_to(of_prompt(new_gate, s), (8, 32))
        input_new = picked(gate_rows, head)
        forget_new = log_sigmoid(picked(gate_rows, 16 + head) + bias_own)
        fresh_terms.append((q_rows, agreement, value_own, input_new, forget_new))

    got = recv_s.at[pl.ds(0, SP - 1)]
    pltpu.make_async_copy(got, got, sems.at[7]).wait()
    pltpu.make_async_copy(got, got, ssem).wait()
    arrived = recv_s[:, 0, :]
    later = (iota((SP, SP), 1) > iota((SP, SP), 0)).astype(F32).astype(BF16)
    sums = jnp.dot(later, jnp.concatenate(split3(arrived), axis=1).astype(BF16), preferred_element_type=F32)
    lw = sums[:, 0:128] + sums[:, 128:256] + sums[:, 256:384] + pltpu.roll(arrived, 64, 1)
    top = jnp.max(lw, axis=0, keepdims=True)
    scale = jnp.exp(lw - top)
    stacked = jnp.concatenate([scale, jnp.broadcast_to(top, (8, 128))], axis=0)
    turned = stacked.T

    factor = DH ** (-0.5)
    lane8 = iota((8, 128), 1)
    for s in range(2):
        q_rows, agreement, value_own, input_new, forget_new = fresh_terms[s]
        top_col = turned[8 * s:8 * s + 8, SP:SP + 1]
        share = turned[8 * s:8 * s + 8, 0:SP]
        top_next = jnp.maximum(forget_new + top_col, input_new)
        old_share = jnp.exp(forget_new + top_col - top_next)
        new_share = jnp.exp(input_new - top_next)
        shares = [jnp.broadcast_to(share[:, d:d + 1], (8, 128)) for d in range(SP)]
        scales = [jnp.broadcast_to(scale[:, 8 * s + 4 * h:8 * s + 4 * h + 1], (SP, 128)) for h in range(2)]
        got = recv_m[s].at[pl.ds(0, SP - 1)]
        pltpu.make_async_copy(got, got, sems.at[3 + s]).wait()
        pltpu.make_async_copy(got, got, msem.at[s]).wait()
        got = recv_n[s].at[pl.ds(0, SP - 1)]
        pltpu.make_async_copy(got, got, sems.at[5 + s]).wait()
        pltpu.make_async_copy(got, got, nsem.at[s]).wait()
        merged = [jnp.zeros((8, 128), F32) for _ in range(4)]
        for d in range(SP):
            merged[d % 4] = merged[d % 4] + shares[d] * recv_m[s][d].astype(F32)
        merged = (merged[0] + merged[1]) + (merged[2] + merged[3])
        matrix = merged.astype(BF16)
        n_rows = []
        for h in range(2):
            normal = jnp.sum(scales[h] * recv_n[s][:, h, :], axis=0, keepdims=True)
            n_rows.append(jnp.broadcast_to(normal, (4, 128)))
        n_rows = jnp.concatenate(n_rows, axis=0)
        numer = jnp.sum(matrix.astype(F32) * q_rows, axis=1, keepdims=True)
        numer = (old_share * numer + new_share * agreement * value_own) * factor
        denom = jnp.sum(n_rows * q_rows, axis=1, keepdims=True)
        denom = (old_share * denom + new_share * agreement) * factor
        read = numer / jnp.maximum(jnp.abs(denom), 1.0)
        own_normal = picked(n_rows, own_row)
        at = pl.ds(pl.multiple_of(8 * order[s], 8), 8)
        table[at, :] = jnp.where(lane8 == 0, own_normal, jnp.where(lane8 == 1, top_col, read))
        packed_out[at, :] = merged
    packed_out[16:24, 0:16] = table[...].T[0:8]


def unpack(packed, mat_out, nrm_out, top_out, read_out):
    for q in range(4):
        s, h = q // 2, q % 2
        lanes = slice(4 * q, 4 * q + 4)
        mat_out[s, h] = packed[lanes].astype(BF16)
        nrm_out[s, h:h + 1, :] = packed[16:17, lanes]
        top_out[s:s + 1, h:h + 1] = packed[17:18, 4 * q:4 * q + 1]
        read_out[s, h:h + 1, :] = packed[18:19, lanes].astype(BF16)


def shards(inputs, w_key, w_value, w_query, w_igate, w_fgate, forget_bias, new_rows):
    seqs, span, width = inputs.shape
    rows = seqs * span
    heads = w_key.shape[1] // DH
    out_shape = (
        jax.ShapeDtypeStruct((seqs, heads, DH // SP, DH), BF16),
        jax.ShapeDtypeStruct((seqs, heads, DH // SP), F32),
        jax.ShapeDtypeStruct((seqs, heads), F32),
        jax.ShapeDtypeStruct((seqs, heads, DH // SP), BF16),
    )
    hbm = pl.BlockSpec(memory_space=pl.ANY)
    vmem = pl.BlockSpec(memory_space=pltpu.VMEM)
    dma = pltpu.SemaphoreType.DMA
    packed = pl.pallas_call(
        kernel,
        out_shape=pltpu.VMEM((24, 128), F32),
        in_specs=[hbm] * 8,
        out_specs=vmem,
        scratch_shapes=[
            [pltpu.VMEM((ROWS, width), BF16) for _ in range(rows // ROWS)],
            pltpu.VMEM((span, width), BF16),
            pltpu.VMEM((2, width, heads * DH), BF16),
            pltpu.VMEM((width, heads * DH), BF16),
            pltpu.VMEM((32, width), BF16),
            pltpu.VMEM((1, 16), F32),
            pltpu.VMEM((TP, seqs, width // TP), BF16),
            pltpu.VMEM((span, 128), F32),
            pltpu.VMEM((span, span), BF16),
            pltpu.VMEM((16, span + 256), F32),
            pltpu.VMEM((2, span + 256), F32),
            pltpu.VMEM((2, span + 256), F32),
            pltpu.VMEM((16, 128), F32),
            [pltpu.VMEM((SP // 2, 2, MSG, 128), BF16) for _ in range(seqs)],
            [pltpu.VMEM((SP, MSG, 128), BF16) for _ in range(seqs)],
            [pltpu.VMEM((2, 128), F32) for _ in range(seqs)],
            [pltpu.VMEM((SP, 2, 128), F32) for _ in range(seqs)],
            pltpu.VMEM((1, 128), F32),
            pltpu.VMEM((SP, 1, 128), F32),
            dma((10,)),
            dma,
            dma,
            dma((seqs,)),
            dma((seqs,)),
            dma,
        ],
        compiler_params=pltpu.CompilerParams(
            collective_id=0, has_side_effects=True, vmem_limit_bytes=60 * 1024 * 1024
        ),
    )(
        inputs.reshape(rows, width), w_key, w_value, w_query,
        w_igate.T, w_fgate.T, forget_bias.reshape(1, -1), new_rows,
    )
    return pl.pallas_call(unpack, out_shape=out_shape, in_specs=[vmem], out_specs=[vmem] * 4)(
        pltpu.with_memory_space_constraint(packed, pltpu.VMEM)
    )


def solution(mesh):
    in_specs = (
        P(None, "sp", None),
        P(None, "tp"),
        P(None, "tp"),
        P(None, "tp"),
        P(),
        P(),
        P(),
        P(None, "tp"),
    )
    out_specs = (P(None, "tp", "sp", None), P(None, "tp", "sp"), P(None, "tp"), P(None, "tp", "sp"))
    return jax.shard_map(shards, mesh=mesh, in_specs=in_specs, out_specs=out_specs, check_vma=False)
```
